256 devices in a mesh: kv: 16 (over y, x), tp: 16 (over z, core).
Axes of the slice: x: 4, y: 4, z: 8, core: 2. Of those that a mesh axis runs over, the one named last changes fastest.
Arguments:
- tokens: bfloat16 [1024, 4096], P('tp', 'kv'), may hold values from -19 to 19, as said below
- lengths: int32 [1024], P('kv'), may hold values from 1 to 16384, 4194304 in all
- state_block: float32 [1024, 64, 2048], P('kv', None, 'tp'), may hold values from -6 to 6
- cached_keys: bfloat16 [1024, 128, 2048], P('kv', None, 'tp'), may hold values from -0.75 to 0.75
- cached_values: bfloat16 [1024, 128, 2048], P('kv', None, 'tp'), may hold values from -6 to 6
- query_weight: bfloat16 [4096, 2048], P('kv', 'tp'), may hold values from -0.09375 to 0.09375
- key_weight: bfloat16 [4096, 2048], P('kv', 'tp'), may hold values from -0.09375 to 0.09375
- value_weight: bfloat16 [4096, 2048], P('kv', 'tp'), may hold values from -0.09375 to 0.09375
- gate_weight: bfloat16 [4096, 2048], P('kv', 'tp'), may hold values from -0.09375 to 0.09375
- decay_rate: float32 [32], P('tp'), may hold values from 0.0005 to 0.05
- head_gain: float32 [2048], P('tp'), may hold values from 0.1 to 1.9
- out_weight: bfloat16 [2048, 4096], P('tp', 'kv'), may hold values from -0.125 to 0.125
- mixer_gain: float32 [4096], P('kv'), may hold values from 0.1 to 1.9
- up_weight: bfloat16 [4096, 16384], P('kv', 'tp'), may hold values from -0.09375 to 0.09375
- down_weight: bfloat16 [16384, 4096], P('tp', 'kv'), may hold values from -0.046875 to 0.046875
- final_gain: float32 [4096], P('kv'), may hold values from 0.1 to 1.9
Outputs:
- next_rows: bfloat16 [1024, 4096], P('tp', 'kv')
The draws below stay inside these ranges and needn't reach their ends.
Inputs may be any that keep to these rules, and one draw needn't show every extreme that they name: `tokens`: the rows' column groups have scales that differ between groups.
All inputs are finite; a program needn't handle non-finite values. No bound on the sum of `lengths` on one device may be relied on, other than what follows from the above.
Results may differ from the reference program's by a relative error of at most 0.0095.
Values may be sent and summed in bfloat16 or wider, within the bound.
A program may use at most 64 MiB of HBM per device.

```python
import math
import jax
import jax.numpy as jnp
import numpy as np
from jax import lax

D = 4096
HEADS = 32
HDIM = 64
FF = 16384
SEQ_DEV = 64
BLK = 128
LEN_MOST = 16384
RW = 2048
ROWS = 1024
LEN_TOTAL = 4194304


def draw_tokens(key, part):
    base, group_key = jax.random.split(jax.random.fold_in(key, 11))
    groups = max(D // 256, 1)
    scales = jnp.exp(jax.random.uniform(group_key, (groups,), jnp.float32, -1.1, 1.1))
    column = jnp.repeat(scales, D // groups, total_repeat_length=D)
    values = jnp.clip(jax.random.normal(base, (ROWS, D), jnp.float32), -6.0, 6.0)
    return (values * column[None, :]).astype(jnp.bfloat16)


def levels(stream_key, dims, cuts, smallest, top_value):
    level, own = 1.0, jax.random.fold_in(stream_key, 6)
    for dim, shards_of in cuts:
        heights = jnp.exp(jax.random.uniform(jax.random.fold_in(own, dim), (shards_of,), jnp.float32, smallest / len(cuts), top_value / len(cuts)))
        level = level * jnp.repeat(heights, dims[dim] // shards_of).reshape([-1 if axis == dim else 1 for axis in range(len(dims))])
    return level


def profile(number_of, total, most, lean):
    weights = [(1 << 20) // math.isqrt(rank ** lean) + 1 for rank in range(2, number_of + 1)]
    spare, counts = total - most - (number_of - 1), [1] * (number_of - 1)
    while spare > 0:
        candidates = [i for i in range(number_of - 1) if counts[i] < most]
        mass, remaining = sum([weights[i] for i in candidates]), spare
        for i in candidates:
            extra = min(most - counts[i], max(1, remaining * weights[i] // mass), spare)
            counts[i] = counts[i] + extra
            spare = spare - extra
    return np.array([most] + counts)


def ragged(key, number_of, total, bound, skew):
    if number_of == 2:
        one = jax.random.randint(key, (), max(1, total - bound), min(bound, total - 1) + 1)
        return jnp.stack([one, total - one])
    tallies = jnp.asarray(profile(number_of, total, bound, skew), jnp.int32)
    pairs = (number_of - 1) // 2
    giver, receiver = tallies[1:1 + 2 * pairs:2], tallies[2:2 + 2 * pairs:2]
    slack = jnp.minimum(giver - 1, bound - receiver)
    passed = jax.random.randint(jax.random.fold_in(key, 1), (pairs,), 0, 1 << 20) % (slack + 1)
    tallies = tallies.at[1:1 + 2 * pairs:2].set(giver - passed).at[2:2 + 2 * pairs:2].set(receiver + passed)
    return tallies[jax.random.permutation(jax.random.fold_in(key, 2), number_of)]


def bell_draw(rng, shape, scale, bound, cuts=(), kind=jnp.bfloat16):
    level = levels(rng, shape, cuts, -0.22, 0.18) if cuts else 1.0
    entries = jax.random.normal(rng, shape, jnp.float32) * scale * level
    return jnp.minimum(jnp.maximum(entries, -bound), bound).astype(kind)


def setup_inputs(seed: int = 0) -> dict:
    seeds = jax.random.split(jax.random.key(seed), 17)
    tokens = draw_tokens(jax.random.fold_in(seeds[16], 71), 0)
    lengths = ragged(seeds[1], ROWS, LEN_TOTAL, LEN_MOST, 2).astype(jnp.int32)
    state_block = bell_draw(seeds[2], (ROWS, HDIM, RW), 1.0, 6.0, ((0, 16), (2, 16)), jnp.float32)
    cached_keys = bell_draw(seeds[3], (ROWS, BLK, RW), 0.125, 0.75, ((0, 16), (2, 16)))
    cached_values = bell_draw(seeds[4], (ROWS, BLK, RW), 1.0, 6.0, ((0, 16), (2, 16)))
    query_weight = bell_draw(seeds[5], (D, RW), D ** -0.5, 0.09375, ((0, 16), (1, 16)))
    key_weight = bell_draw(seeds[6], (D, RW), D ** -0.5, 0.09375, ((0, 16), (1, 16)))
    value_weight = bell_draw(seeds[7], (D, RW), D ** -0.5, 0.09375, ((0, 16), (1, 16)))
    gate_weight = bell_draw(seeds[8], (D, RW), D ** -0.5, 0.09375, ((0, 16), (1, 16)))
    decay_rate = jnp.clip(jnp.exp(math.log(0.05) - 4.6051702 * jax.random.uniform(seeds[9], (HEADS,), jnp.float32) ** levels(seeds[9], (HEADS,), ((0, 16),), -0.2, 0.2)), 0.0005, 0.05)
    head_gain = jnp.clip(1.0 + 0.18 * jax.random.normal(seeds[10], (RW,), jnp.float32), 0.1, 1.9)
    out_weight = bell_draw(seeds[11], (RW, D), RW ** -0.5, 0.125, ((0, 16), (1, 16)))
    mixer_gain = jnp.clip(1.0 + 0.18 * jax.random.normal(seeds[12], (D,), jnp.float32), 0.1, 1.9)
    up_weight = bell_draw(seeds[13], (D, FF), D ** -0.5, 0.09375, ((0, 16), (1, 16)))
    down_weight = bell_draw(seeds[14], (FF, D), FF ** -0.5, 0.046875, ((0, 16), (1, 16)))
    final_gain = jnp.clip(1.0 + 0.18 * jax.random.normal(seeds[15], (D,), jnp.float32), 0.1, 1.9)
    return {"tokens": tokens, "lengths": lengths, "state_block": state_block, "cached_keys": cached_keys, "cached_values": cached_values, "query_weight": query_weight, "key_weight": key_weight, "value_weight": value_weight, "gate_weight": gate_weight, "decay_rate": decay_rate, "head_gain": head_gain, "out_weight": out_weight, "mixer_gain": mixer_gain, "up_weight": up_weight, "down_weight": down_weight, "final_gain": final_gain}


ALPHA = 2.0 ** 0.5
EPS = 1e-05

def rotate(vectors, positions):
    half = vectors.shape[-1] // 2
    inverse = 10000.0 ** (-jnp.arange(half, dtype=jnp.float32) / half)
    angle = positions.astype(jnp.float32)[:, None] * inverse[None, :]
    cosine = jnp.cos(angle)[:, None, :]
    sine = jnp.sin(angle)[:, None, :]
    former, latter = (vectors[..., :half], vectors[..., half:])
    return jnp.concatenate([former * cosine - latter * sine, latter * cosine + former * sine], -1)

def layer_norm(values, gain):
    mean = lax.optimization_barrier(jnp.mean(values, 1, keepdims=True))
    centred = values - mean
    spread = lax.optimization_barrier(jnp.mean(centred * centred, 1, keepdims=True))
    return centred * lax.rsqrt(spread + EPS) * gain[None, :]

def retain(query, keyed, valued, gated, lengths, state, keys, values, rate, gain):
    count = query.shape[0]
    heads = rate.shape[0]
    q_rot = rotate(query.astype(jnp.float32).reshape(count, heads, HDIM), lengths).astype(jnp.bfloat16)
    k_rot = (rotate(keyed.astype(jnp.float32).reshape(count, heads, HDIM), lengths) * 0.125).astype(jnp.bfloat16)
    v_new = valued.astype(jnp.float32).reshape(count, heads, HDIM)
    cached_k = keys.astype(jnp.float32).reshape(count, BLK, heads, HDIM)
    cached_v = values.astype(jnp.float32).reshape(count, BLK, heads, HDIM)
    q_wide = q_rot.astype(jnp.float32)
    scores = jnp.einsum('shn,sihn->shi', q_wide, cached_k)
    offset = lengths % BLK
    slots = jnp.arange(BLK, dtype=jnp.int32)
    lag = jnp.maximum(offset[:, None] - slots[None, :], 0).astype(jnp.float32)
    live = (slots[None, :] < offset[:, None])[:, None, :]
    factor = jnp.where(live, jnp.exp(-rate[None, :, None] * lag[:, None, :]), 0.0)
    weights = (scores * factor).astype(jnp.bfloat16).astype(jnp.float32)
    own = lax.optimization_barrier(jnp.sum(q_wide * k_rot.astype(jnp.float32), -1)).astype(jnp.bfloat16).astype(jnp.float32)
    inner = jnp.einsum('shi,sihn->shn', weights, cached_v) + own[..., None] * v_new
    carried = jnp.exp(-rate[None, :] * (offset[:, None] + 1).astype(jnp.float32))
    cross = jnp.einsum('shk,skhv->shv', q_wide, state.reshape(count, HDIM, heads, HDIM), precision=lax.Precision.HIGHEST) * carried[..., None]
    retained = inner + cross
    mean = lax.optimization_barrier(jnp.mean(retained, -1, keepdims=True))
    centred = retained - mean
    spread = lax.optimization_barrier(jnp.mean(centred * centred, -1, keepdims=True))
    normed = centred * lax.rsqrt(spread + EPS) * gain.reshape(heads, HDIM)[None]
    gate_f = jax.nn.silu(gated.astype(jnp.float32).reshape(count, heads, HDIM))
    return (gate_f * normed).reshape(count, heads * HDIM).astype(jnp.bfloat16)

def reference(tokens, lengths, state_block, cached_keys, cached_values, query_weight, key_weight, value_weight, gate_weight, decay_rate, head_gain, out_weight, mixer_gain, up_weight, down_weight, final_gain):
    projected = [jnp.dot(tokens, weight, preferred_element_type=jnp.float32).astype(jnp.bfloat16) for weight in (query_weight, key_weight, value_weight, gate_weight)]
    blocks = ROWS // SEQ_DEV

    def split_rows(array):
        return array.reshape((blocks, SEQ_DEV) + array.shape[1:])

    def one_block(items):
        query, keyed, valued, gated, length_rows, state, keys, values = items
        return retain(query, keyed, valued, gated, length_rows, state, keys, values, decay_rate, head_gain)
    mixed = lax.map(one_block, tuple((split_rows(array) for array in projected + [lengths, state_block, cached_keys, cached_values])))
    mixed = mixed.reshape(ROWS, RW)
    branch = jnp.dot(mixed, out_weight, preferred_element_type=jnp.float32)
    hidden = layer_norm(ALPHA * tokens.astype(jnp.float32) + branch, mixer_gain).astype(jnp.bfloat16)
    upward = jnp.dot(hidden, up_weight, preferred_element_type=jnp.float32)
    active = jnp.square(jax.nn.relu(upward)).astype(jnp.bfloat16)
    downward = jnp.dot(active, down_weight, preferred_element_type=jnp.float32)
    return layer_norm(ALPHA * hidden.astype(jnp.float32) + downward, final_gain).astype(jnp.bfloat16)
```

```python
import functools

import jax
import jax.numpy as jnp
from jax import lax
from jax.sharding import Mesh
from jax.sharding import PartitionSpec as P

HDIM = 64
BLK = 128
KV = ("kv_0", "kv_1")


ALPHA = 2.0**0.5
EPS = 1e-05


def by_axis(x, axes):
    return functools.reduce(lax.psum, axes, x)


def copy_for_each(x, axis):
    peers = lax.axis_size(axis)
    return lax.all_to_all(jnp.broadcast_to(x[None], (peers, *x.shape)), axis, 0, 0, tiled=True)


def joined_along(parts, dim):
    parts = jnp.moveaxis(parts, 0, dim)
    dims = parts.shape
    return parts.reshape(*dims[:dim], dims[dim] * dims[dim + 1], *dims[dim + 2 :])


def gather_directly(x, axis, dim):
    parts = copy_for_each(x, axis)
    return joined_along(parts, dim)


def split_up(x, dim, peers):
    dims = x.shape
    parts = x.reshape(*dims[:dim], peers, dims[dim] // peers, *dims[dim + 1 :])
    return jnp.moveaxis(parts, dim, 0)


def sent_and_summed(x, axis, dim):
    parts = split_up(x, dim, lax.axis_size(axis)).astype(jnp.bfloat16)
    arrived = lax.all_to_all(parts, axis, split_axis=0, concat_axis=0, tiled=True)
    return arrived.astype(jnp.float32).sum(axis=0)


def rotate(vectors, positions):
    half = vectors.shape[-1] // 2
    inverse = 10000.0 ** (-jnp.arange(half, dtype=jnp.float32) / half)
    angle = positions.astype(jnp.float32)[:, None] * inverse[None, :]
    cosine = jnp.cos(angle)[:, None, :]
    sine = jnp.sin(angle)[:, None, :]
    former, latter = (vectors[..., :half], vectors[..., half:])
    return jnp.concatenate([former * cosine - latter * sine, latter * cosine + former * sine], -1)


def normalize(values, gain):
    width = values.shape[1] * lax.axis_size(KV)
    sums = jnp.stack([jnp.sum(values, 1), jnp.sum(values * values, 1)])
    total, square = copy_for_each(sums, KV).sum(axis=0)
    mean = total / width
    centred = values - mean[:, None]
    spread = square / width - mean * mean
    return centred * lax.rsqrt(spread[:, None] + EPS) * gain[None, :]


def retain(query, keyed, valued, gated, lengths, state, keys, values, rate, gain):
    count = query.shape[0]
    heads = rate.shape[0]
    q_rot = rotate(query.astype(jnp.float32).reshape(count, heads, HDIM), lengths).astype(
        jnp.bfloat16
    )
    k_rot = (rotate(keyed.astype(jnp.float32).reshape(count, heads, HDIM), lengths) * 0.125).astype(
        jnp.bfloat16
    )
    v_new = valued.astype(jnp.float32).reshape(count, heads, HDIM)
    cached_k = keys.reshape(count, BLK, heads, HDIM)
    cached_v = values.reshape(count, BLK, heads, HDIM)
    scores = jnp.einsum("shn,sihn->shi", q_rot, cached_k, preferred_element_type=jnp.float32)
    offset = lengths % BLK
    slots = jnp.arange(BLK, dtype=jnp.int32)
    lag = jnp.maximum(offset[:, None] - slots[None, :], 0).astype(jnp.float32)
    live = (slots[None, :] < offset[:, None])[:, None, :]
    factor = jnp.where(live, jnp.exp(-rate[None, :, None] * lag[:, None, :]), 0.0)
    weights = (scores * factor).astype(jnp.bfloat16)
    own = jnp.einsum("shn,shn->sh", q_rot, k_rot, preferred_element_type=jnp.float32).astype(
        jnp.bfloat16
    )
    inner = jnp.einsum("shi,sihn->shn", weights, cached_v, preferred_element_type=jnp.float32)
    inner = inner + own.astype(jnp.float32)[..., None] * v_new
    carried = jnp.exp(-rate[None, :] * (offset[:, None] + 1).astype(jnp.float32))
    cross = (
        jnp.einsum(
            "shk,skhv->shv", q_rot.astype(jnp.float32), state.reshape(count, HDIM, heads, HDIM)
        )
        * carried[..., None]
    )
    retained = inner + cross
    mean = jnp.mean(retained, -1, keepdims=True)
    centred = retained - mean
    spread = jnp.mean(centred * centred, -1, keepdims=True)
    normed = centred * lax.rsqrt(spread + EPS) * gain.reshape(heads, HDIM)[None]
    gate_f = jax.nn.silu(gated.astype(jnp.float32).reshape(count, heads, HDIM))
    return (gate_f * normed).reshape(count, heads * HDIM).astype(jnp.bfloat16)


def per_device(
    tokens,
    lengths,
    state_block,
    cached_keys,
    cached_values,
    query_weight,
    key_weight,
    value_weight,
    gate_weight,
    decay_rate,
    head_gain,
    out_weight,
    mixer_gain,
    up_weight,
    down_weight,
    final_gain,
):
    all_rows = gather_directly(tokens, "tp", 0)
    width = query_weight.shape[1]
    piece = all_rows
    summed = sent_and_summed(
        jnp.concatenate(
            [
                jnp.dot(piece, weight, preferred_element_type=jnp.float32)
                for weight in (query_weight, key_weight, value_weight, gate_weight)
            ],
            1,
        ),
        KV,
        0,
    ).astype(jnp.bfloat16)
    query, keyed, valued, gated = [
        summed[:, index * width : (index + 1) * width] for index in range(4)
    ]
    mixed = retain(
        query,
        keyed,
        valued,
        gated,
        lengths,
        state_block,
        cached_keys,
        cached_values,
        decay_rate,
        head_gain,
    )
    mixed_all = gather_directly(mixed, KV, 0)
    piece = mixed_all
    branch = sent_and_summed(
        jnp.dot(piece, out_weight, preferred_element_type=jnp.float32), "tp", 0
    )
    hidden = normalize(ALPHA * tokens.astype(jnp.float32) + branch, mixer_gain).astype(jnp.bfloat16)
    hidden_all = gather_directly(hidden, "tp", 0)
    piece = hidden_all
    upward = sent_and_summed(jnp.dot(piece, up_weight, preferred_element_type=jnp.float32), KV, 0)
    active = jnp.square(jax.nn.relu(upward)).astype(jnp.bfloat16)
    terms = jnp.dot(gather_directly(active, KV, 0), down_weight, preferred_element_type=jnp.float32)
    downward = sent_and_summed(terms, "tp", 0)
    result = normalize(ALPHA * hidden.astype(jnp.float32) + downward, final_gain)
    return result.astype(jnp.bfloat16)


def solution(mesh):
    finer = Mesh(mesh.devices.reshape(4, 4, mesh.shape["tp"]), ("kv_0", "kv_1", "tp"))
    placed = (
        P("tp", KV),
        P(KV),
        P(KV, None, "tp"),
        P(KV, None, "tp"),
        P(KV, None, "tp"),
        P(KV, "tp"),
        P(KV, "tp"),
        P(KV, "tp"),
        P(KV, "tp"),
        P("tp"),
        P("tp"),
        P("tp", KV),
        P(KV),
        P(KV, "tp"),
        P("tp", KV),
        P(KV),
    )
    return jax.shard_map(
        per_device, mesh=finer, in_specs=placed, out_specs=P("tp", KV), check_vma=False
    )
```

```python
import functools

import jax
import jax.numpy as jnp
from jax import lax
from jax.experimental import pallas as pl
from jax.experimental.pallas import tpu as pltpu
from jax.sharding import Mesh
from jax.sharding import PartitionSpec as P

HDIM = 64
BLK = 128
ALPHA = 2.0**0.5
EPS = 1e-05
AXES = ("y", "x", "z", "c")
NEAR = (0, 1, 7, 2, 6, 3, 5, 4)
F32 = jnp.float32
B16 = jnp.bfloat16


def dot(a, b):
    return jnp.dot(a, b, preferred_element_type=F32)


def split_dot(a, b, terms, left=True):
    total = None
    rest = a if left else b
    for _ in range(terms):
        part = rest.astype(B16)
        rest = rest - part.astype(F32)
        term = dot(part, b) if left else dot(a, part)
        total = term if total is None else total + term
    return total


def copy_to(src, dst, send, recv, device):
    return pltpu.make_async_remote_copy(
        src_ref=src,
        dst_ref=dst,
        send_sem=send,
        recv_sem=recv,
        device_id=device,
        device_id_type=pl.DeviceIdType.MESH,
    )


def kernel(
    tok, cosine, sine, offset, rate, head_gain, mixer_gain, final_gain,
    state_h, keys_h, values_h, wq_h, wk_h, wv_h, wg_h, wo_h, wu_h, wd_h,
    out,
    state, keys, values, factor, wp, wo, wu, wd,
    t_all, b_out, b_in, qkvg, retained, mixed, m_all, d_out, d_in,
    s_out, s_in, hidden, h_all, g1_out, g1_in, g2_out, g2_in, act_all, e_out, e_in, f_out, f_in,
    local, send, r_w, r_a, r_b, r_c, r_d, r_e, r_f, r_g1, r_g2, r_h1, r_h2, r_i, r_j,
):
    y, x, z, c = [lax.axis_index(name) for name in AXES]
    kv = y * 4 + x
    sibling = (y, x, z, 1 - c)
    row_of = lax.rem(x, 2)
    owner = row_of == c

    def arrived(dst, sem):
        copy_to(dst, dst, send.at[0], sem, sibling).wait_recv()

    here = []

    def fetch(src, dst):
        here.append(pltpu.make_async_copy(src, dst, local.at[len(here)]))
        here[-1].start()

    quarter = [wp.at[c, :, pl.ds(128 * i, 128)] for i in range(4)]
    for src, dst in zip((wq_h, wk_h, wv_h, wg_h), quarter):
        fetch(src, dst)
    fetch(wo_h, wo.at[c])
    fetch(wu_h, wu.at[c])
    fetch(wd_h, wd.at[c])
    fetch(keys_h, keys)
    fetch(values_h, values)
    fetch(state_h, state)

    barrier = pltpu.get_barrier_semaphore()
    greeted = 0
    for dy in range(4):
        for dx in range(4):
            for dc in range(2):
                if dy or dx or dc:
                    peer = (lax.rem(y + dy, 4), lax.rem(x + dx, 4), z, lax.rem(c + dc, 2))
                    pl.semaphore_signal(barrier, inc=1, device_id=peer, device_id_type=pl.DeviceIdType.MESH)
                    greeted += 1
    for dz in range(1, 8):
        peer = (y, x, lax.rem(z + dz, 8), c)
        pl.semaphore_signal(barrier, inc=1, device_id=peer, device_id_type=pl.DeviceIdType.MESH)
        greeted += 1

    def decay(i, carry):
        rows = pl.ds(pl.multiple_of(i * 8, 8), 8)
        off = offset[rows, :][:, None, :]
        slot = lax.broadcasted_iota(jnp.int32, (8, BLK, 128), 1).astype(F32)
        lag = jnp.maximum(off - slot, 0.0)
        factor[rows] = jnp.where(slot < off, jnp.exp(-rate[...][None] * lag), 0.0)
        return carry

    lax.fori_loop(0, 8, decay, 0)
    t_all[z] = tok[...]
    pl.semaphore_wait(barrier, greeted)

    a_sends = []
    for d in NEAR[1:]:
        a_sends.append(copy_to(tok, t_all.at[z], send.at[d], r_a.at[z], (y, x, lax.rem(z + d, 8), c)))
        a_sends[-1].start()
    w_sends = []
    for i, (src, dst) in enumerate(
        [*zip((wq_h, wk_h, wv_h, wg_h), quarter), (wo_h, wo.at[c]), (wu_h, wu.at[c]), (wd_h, wd.at[c])]
    ):
        w_sends.append(copy_to(src, dst, send.at[8 + i], r_w.at[i], sibling))
        w_sends[-1].start()
    theirs = [wp.at[1 - c, :, pl.ds(128 * i, 128)] for i in range(4)] + [w.at[1 - c] for w in (wo, wu, wd)]
    for i in range(4):
        here[i].wait()
        arrived(theirs[i], r_w.at[i])

    b_sends = []
    for d in NEAR:
        zp = lax.rem(z + 8 - d, 8)
        if d:
            arrived(t_all.at[zp], r_a.at[zp])
        block = 2 * zp + c
        rows = t_all[zp]
        for core in range(2):
            part = dot(rows, wp[core]).astype(B16)
            mine = jnp.logical_and(block == kv, c == core)
            b_out[zp, core] = part
            copy = copy_to(
                b_out.at[zp, core], b_in.at[kv], send.at[16 + d * 2 + core], r_b.at[kv],
                (block // 4, lax.rem(block, 4), z, core),
            )
            b_sends.append((jnp.logical_not(mine), copy))

            @pl.when(mine)
            def _():
                b_in[kv] = part

            @pl.when(jnp.logical_not(mine))
            def _():
                copy.start()

    for copy in a_sends + w_sends:
        copy.wait_send()

    def wait_projected(i, carry):
        @pl.when(jnp.logical_not(jnp.logical_and(i == kv, owner)))
        def _():
            arrived(b_in.at[i], r_b.at[i])

        return carry

    lax.fori_loop(0, 16, wait_projected, 0)
    qkvg[...] = b_in[0].astype(F32)

    def add_projected(i, carry):
        qkvg[...] += b_in[i].astype(F32)
        return carry

    lax.fori_loop(1, 16, add_projected, 0)

    lane = lax.broadcasted_iota(jnp.int32, (64, 128), 1)
    low = lax.rem(lane, HDIM) < HDIM // 2
    row_id = lax.broadcasted_iota(jnp.int32, (128, 128), 0)
    col_id = lax.broadcasted_iota(jnp.int32, (128, 128), 1)
    same_head = jnp.where(row_id // HDIM == col_id // HDIM, 1.0, 0.0).astype(B16)

    def rotated(u):
        partner = jnp.where(low, pltpu.roll(u, 96, 1), pltpu.roll(u, 32, 1))
        return u * cosine[...] + partner * sine[...]

    query, keyed, valued, gated = [
        qkvg[:, 128 * i : 128 * (i + 1)].astype(B16).astype(F32) for i in range(4)
    ]
    q_rot = rotated(query).astype(B16).astype(F32)
    k_rot = (rotated(keyed) * 0.125).astype(B16).astype(F32)
    own = split_dot(q_rot * k_rot, same_head, 2).astype(B16).astype(F32)
    mixed[...] = q_rot
    retained[...] = own * valued
    for copy in here[7:]:
        copy.wait()
    pick_lane = lax.broadcasted_iota(jnp.int32, (HDIM, 128), 1)
    pick_row = lax.broadcasted_iota(jnp.int32, (HDIM, 128), 0)
    pick = jnp.where(lax.rem(pick_lane, HDIM) == pick_row, 1.0, 0.0)

    def attend(i, carry):
        rows = pl.ds(pl.multiple_of(i * 8, 8), 8)
        q = mixed[rows, :]
        products = (keys[rows].astype(F32) * q[:, None, :]).reshape(8 * BLK, 128)
        scores = split_dot(products, same_head, 2).reshape(8, BLK, 128)
        weights = (scores * factor[rows]).astype(B16).astype(F32)
        inner = jnp.sum(weights * values[rows].astype(F32), axis=1)
        spread = (q[:, None, :] * pick[None]).reshape(8 * HDIM, 128).astype(B16)
        wide = dot(spread, same_head).reshape(8, HDIM, 128)
        cross = jnp.sum(wide * state[rows], axis=1)
        carried = jnp.exp(-rate[...] * (offset[rows, :] + 1.0))
        retained[rows, :] += inner + cross * carried
        return carry

    lax.fori_loop(0, 8, attend, 0)
    kept = retained[...]
    centred = kept - split_dot(kept, same_head, 3) * (1.0 / HDIM)
    variance = split_dot(centred * centred, same_head, 3) * (1.0 / HDIM)
    normed = centred * lax.rsqrt(variance + EPS) * head_gain[...]
    heads = (gated / (1.0 + jnp.exp(-gated)) * normed).astype(B16)

    for used, copy in b_sends:

        @pl.when(used)
        def _():
            copy.wait_send()

    half = kv // 2
    m_out = d_out.at[0, :, pl.ds(0, 128)]
    d_out[0, :, 0:128] = heads

    @pl.when(owner)
    def _():
        m_all[half, c] = heads

    m_sends = []
    for k in range(16):
        dy, dx = k // 4, k % 4
        to = lax.rem(y + dy, 4), lax.rem(x + dx, 4)
        copy = copy_to(m_out, m_all.at[half, c], send.at[k], r_c.at[half, c], (*to, z, row_of))
        if k:
            copy.start()
        else:

            @pl.when(jnp.logical_not(owner))
            def _():
                copy.start()

        m_sends.append(copy)
    arrived(theirs[4], r_w.at[4])
    here[4].wait()

    for k, copy in enumerate(m_sends):
        if k:
            copy.wait_send()
        else:

            @pl.when(jnp.logical_not(owner))
            def _():
                copy.wait_send()

    d_sends = []
    for d in (4, 3, 5, 2, 6, 1, 7, 0):
        i = lax.rem(z + d, 8)
        for core in range(2):
            @pl.when(jnp.logical_not(jnp.logical_and(2 * i + c == kv, c == core)))
            def _():
                arrived(m_all.at[i, core], r_c.at[i, core])
        part = dot(m_all[i, 0], wo[0]) + dot(m_all[i, 1], wo[1])
        if d:
            d_out[i] = part.astype(B16)
            copy = copy_to(d_out.at[i], d_in.at[z], send.at[d], r_d.at[z], (y, x, i, c))
            copy.start()
            d_sends.append(copy)
        else:
            branch = part
    for d in NEAR[1:]:
        i = lax.rem(z + 8 - d, 8)
        arrived(d_in.at[i], r_d.at[i])
        branch = branch + d_in[i].astype(F32)
    for copy in d_sends:
        copy.wait_send()

    ones = jnp.full((8, 256), 1.0, B16)
    first = jnp.where(lax.broadcasted_iota(jnp.int32, (8, 256), 0) == 0, 1.0, 0.0).astype(B16)

    def row_sums(u):
        total = None
        for _ in range(3):
            part = u.astype(B16)
            u = u - part.astype(F32)
            term = lax.dot_general(ones, part, (((1,), (1,)), ((), ())), preferred_element_type=F32)
            total = term if total is None else total + term
        return total

    def column(u):
        total = None
        for _ in range(3):
            part = u.astype(B16)
            u = u - part.astype(F32)
            term = lax.dot_general(part, first, (((0,), (0,)), ((), ())), preferred_element_type=F32)
            total = term if total is None else total + term
        return total

    def normalized(values, gain, sums, sums_in, sem):
        sums[0] = row_sums(values)
        sums[1] = row_sums(values * values)
        sums_in[kv] = sums[...]
        copies = []
        for k in range(1, 16):
            to = (lax.rem(y + k // 4, 4), lax.rem(x + k % 4, 4), z, c)
            copies.append(copy_to(sums, sums_in.at[kv], send.at[k], sem.at[kv], to))
            copies[-1].start()
        for k in range(1, 16):
            i = lax.rem(y + k // 4, 4) * 4 + lax.rem(x + k % 4, 4)
            arrived(sums_in.at[i], sem.at[i])
        total = jnp.sum(sums_in[:, 0], axis=0) * (1.0 / 4096)
        square = jnp.sum(sums_in[:, 1], axis=0) * (1.0 / 4096)
        for copy in copies:
            copy.wait_send()
        scale = lax.rsqrt(square - total * total + EPS)
        return (values - column(total)) * column(scale) * gain[...]

    tall = ALPHA * tok[...].astype(F32) + branch
    rows_now = normalized(tall, mixer_gain, s_out, s_in, r_e).astype(B16)
    hidden[...] = rows_now
    h_all[z] = rows_now

    h_sends = []
    for d in NEAR[1:]:
        h_sends.append(copy_to(hidden, h_all.at[z], send.at[d], r_f.at[z], (y, x, lax.rem(z + d, 8), c)))
        h_sends[-1].start()
    for i in (5, 6):
        here[i].wait()
        arrived(theirs[i], r_w.at[i])

    def up_block(d, carry):
        zp = lax.rem(z + 8 - d, 8)

        @pl.when(d > 0)
        def _():
            arrived(h_all.at[zp], r_f.at[zp])

        yd = zp // 2
        xd = lax.rem(zp, 2) * 2
        rows = h_all[zp]
        first_half = dot(rows, wu[0]).astype(B16)
        second_half = dot(rows, wu[1]).astype(B16)
        for side in range(2):
            to_x = xd + side
            g1_out[0, to_x, yd] = first_half[32 * side : 32 * side + 32]
            g1_out[1, yd, to_x] = second_half[32 * side : 32 * side + 32]

        return carry

    for d in NEAR:
        up_block(d, 0)
    for copy in h_sends:
        copy.wait_send()

    along = (x, y)

    def device_on(colour, stage, index):
        if (colour + stage) % 2 == 0:
            return (y, index, z, c)
        return (index, x, z, c)

    g1_sends = []
    for j in (1, 3, 2, 0):
        for d in (2, 1, 3):
            for colour in range(2):
                me, other = along[colour], along[1 - colour]
                to, piece = lax.rem(me + d, 4), lax.rem(other + j, 4)
                copy = copy_to(
                    g1_out.at[colour, to, piece], g1_in.at[colour, me, piece],
                    send.at[len(g1_sends)], r_g1.at[colour, me, piece], device_on(colour, 0, to),
                )
                copy.start()
                g1_sends.append(copy)
    g2_sends = []
    for j in (1, 3, 2, 0):
        for colour in range(2):
            me, other = along[colour], along[1 - colour]
            piece = lax.rem(other + j, 4)
            total = g1_out[colour, me, piece].astype(F32)
            for d in (1, 3, 2):
                source = lax.rem(me + d, 4)
                arrived(g1_in.at[colour, source, piece], r_g1.at[colour, source, piece])
                total = total + g1_in[colour, source, piece].astype(F32)
            if j:
                g2_out[colour, piece] = total.astype(B16)
                copy = copy_to(
                    g2_out.at[colour, piece], g2_in.at[colour, other],
                    send.at[24 + len(g2_sends)], r_g2.at[colour, other], device_on(colour, 1, piece),
                )
                copy.start()
                g2_sends.append(copy)
            else:
                f_out[colour] = total
    for copy in g1_sends:
        copy.wait_send()

    def place(colour, i, j):
        if colour == 0:
            return (colour, i, j)
        return (colour, j, i)

    h1_sends = []
    h2_sends = []
    for colour in range(2):
        me, other = along[colour], along[1 - colour]
        total = f_out[colour]
        for d in (1, 3, 2):
            source = lax.rem(other + d, 4)
            arrived(g2_in.at[colour, source], r_g2.at[colour, source])
            total = total + g2_in[colour, source].astype(F32)
        active = jnp.square(jnp.maximum(total, 0.0)).astype(B16)
        spot = act_all.at[colour, y, x]
        act_all[colour, y, x] = active
        for d in (2, 1, 3):
            to = lax.rem(other + d, 4)
            copy = copy_to(
                spot, spot, send.at[len(h1_sends)], r_h1.at[colour, other], device_on(colour, 1, to)
            )
            copy.start()
            h1_sends.append(copy)
        for d in (2, 1, 3):
            to = lax.rem(me + d, 4)
            copy = copy_to(
                spot, spot, send.at[6 + len(h2_sends)], r_h2.at[colour, other, me], device_on(colour, 0, to)
            )
            copy.start()
            h2_sends.append(copy)
    for copy in g2_sends:
        copy.wait_send()
    for j in (1, 3, 2):
        for colour in range(2):
            me, other = along[colour], along[1 - colour]
            source = lax.rem(other + j, 4)
            spot = act_all.at[place(colour, source, me)]
            arrived(spot, r_h1.at[colour, source])
            for d in (2, 1, 3):
                to = lax.rem(me + d, 4)
                copy = copy_to(
                    spot, spot, send.at[6 + len(h2_sends)], r_h2.at[colour, source, me],
                    device_on(colour, 0, to),
                )
                copy.start()
                h2_sends.append(copy)
    for j in (0, 1, 3, 2):
        for d in (1, 3, 2):
            for colour in range(2):
                me, other = along[colour], along[1 - colour]
                source, at = lax.rem(other + j, 4), lax.rem(me + d, 4)
                arrived(act_all.at[place(colour, source, at)], r_h2.at[colour, source, at])
    for copy in h1_sends + h2_sends:
        copy.wait_send()

    e_sends = []
    for d in (4, 3, 5, 2, 6, 1, 7, 0):
        i = lax.rem(z + d, 8)
        yd, xd = i // 2, lax.rem(i, 2) * 2
        part = None
        for colour in range(2):
            rows = act_all[colour, yd, pl.ds(xd, 2)].reshape(64, 1024)
            term = dot(rows, wd[colour])
            part = term if part is None else part + term
        if d:
            e_out[i] = part.astype(B16)
            copy = copy_to(e_out.at[i], e_in.at[z], send.at[d], r_i.at[z], (y, x, i, c))
            copy.start()
            e_sends.append(copy)
        else:
            downward = part
    for d in NEAR[1:]:
        i = lax.rem(z + 8 - d, 8)
        arrived(e_in.at[i], r_i.at[i])
        downward = downward + e_in[i].astype(F32)
    for copy in e_sends:
        copy.wait_send()
    tall = ALPHA * hidden[...].astype(F32) + downward
    out[...] = normalized(tall, final_gain, s_out, f_in, r_j).astype(B16)


def per_device(
    tokens, lengths, state_block, cached_keys, cached_values, query_weight, key_weight,
    value_weight, gate_weight, decay_rate, head_gain, out_weight, mixer_gain, up_weight,
    down_weight, final_gain,
):
    half = HDIM // 2
    inverse = 10000.0 ** (-jnp.arange(half, dtype=F32) / half)
    angle = lengths.astype(F32)[:, None] * inverse[None, :]
    cosine, sine = jnp.cos(angle), jnp.sin(angle)
    cosine = jnp.concatenate([cosine] * 4, 1)
    sine = jnp.concatenate([-sine, sine] * 2, 1)
    offset = jnp.broadcast_to((lengths % BLK).astype(F32)[:, None], (64, 128))
    rate = jnp.repeat(decay_rate, HDIM)[None, :]
    vmem = pl.BlockSpec(memory_space=pltpu.VMEM)
    anywhere = pl.BlockSpec(memory_space=pl.ANY)
    dma = pltpu.SemaphoreType.DMA
    scratch = [
        pltpu.VMEM((64, 64, 128), F32),
        pltpu.VMEM((64, 128, 128), B16),
        pltpu.VMEM((64, 128, 128), B16),
        pltpu.VMEM((64, 128, 128), F32),
        pltpu.VMEM((2, 256, 512), B16),
        pltpu.VMEM((2, 128, 256), B16),
        pltpu.VMEM((2, 256, 1024), B16),
        pltpu.VMEM((2, 1024, 256), B16),
        pltpu.VMEM((8, 64, 256), B16),
        pltpu.VMEM((8, 2, 64, 512), B16),
        pltpu.VMEM((16, 64, 512), B16),
        pltpu.VMEM((64, 512), F32),
        pltpu.VMEM((64, 128), F32),
        pltpu.VMEM((64, 128), F32),
        pltpu.VMEM((8, 2, 64, 128), B16),
        pltpu.VMEM((8, 64, 256), B16),
        pltpu.VMEM((8, 64, 256), B16),
        pltpu.VMEM((2, 8, 64), F32),
        pltpu.VMEM((16, 2, 8, 64), F32),
        pltpu.VMEM((64, 256), B16),
        pltpu.VMEM((8, 64, 256), B16),
        pltpu.VMEM((2, 4, 4, 32, 1024), B16),
        pltpu.VMEM((2, 4, 4, 32, 1024), B16),
        pltpu.VMEM((2, 4, 32, 1024), B16),
        pltpu.VMEM((2, 4, 32, 1024), B16),
        pltpu.VMEM((2, 4, 4, 32, 1024), B16),
        pltpu.VMEM((8, 64, 256), B16),
        pltpu.VMEM((8, 64, 256), B16),
        pltpu.VMEM((2, 32, 1024), F32),
        pltpu.VMEM((16, 2, 8, 64), F32),
        dma((10,)),
        dma((40,)),
        dma((7,)),
        dma((8,)),
        dma((16,)),
        dma((8, 2)),
        dma((8,)),
        dma((16,)),
        dma((8,)),
        dma((2, 4, 4)),
        dma((2, 4)),
        dma((2, 4)),
        dma((2, 4, 4)),
        dma((8,)),
        dma((16,)),
    ]
    return pl.pallas_call(
        kernel,
        out_shape=jax.ShapeDtypeStruct((64, 256), B16),
        in_specs=[vmem] * 8 + [anywhere] * 10,
        out_specs=vmem,
        scratch_shapes=scratch,
        name="layer",
        compiler_params=pltpu.CompilerParams(
            collective_id=0, has_side_effects=True, vmem_limit_bytes=56 * 1024 * 1024
        ),
    )(
        tokens, cosine, sine, offset, rate, head_gain[None, :], mixer_gain[None, :], final_gain[None, :],
        state_block, cached_keys, cached_values, query_weight, key_weight, value_weight, gate_weight,
        out_weight, up_weight, down_weight,
    )


def solution(mesh):
    finer = Mesh(mesh.devices.reshape(4, 4, 8, 2), AXES)
    kv, tp = ("y", "x"), ("z", "c")
    placed = (
        P(tp, kv), P(kv), P(kv, None, tp), P(kv, None, tp), P(kv, None, tp),
        P(kv, tp), P(kv, tp), P(kv, tp), P(kv, tp), P(tp), P(tp), P(tp, kv), P(kv),
        P(kv, tp), P(tp, kv), P(kv),
    )
    return jax.shard_map(per_device, mesh=finer, in_specs=placed, out_specs=P(tp, kv), check_vma=False)
```

```python
import functools

import jax
import jax.numpy as jnp
from jax import lax
from jax.experimental import pallas as pl
from jax.experimental.pallas import tpu as pltpu
from jax.sharding import Mesh
from jax.sharding import PartitionSpec as P

HDIM = 64
BLK = 128
ALPHA = 2.0**0.5
EPS = 1e-05
AXES = ("y", "x", "z", "c")
NEAR = (0, 1, 7, 2, 6, 3, 5, 4)
F32 = jnp.float32
B16 = jnp.bfloat16


def dot(a, b):
    return jnp.dot(a, b, preferred_element_type=F32)


def split_dot(a, b, terms, left=True):
    total = None
    rest = a if left else b
    for _ in range(terms):
        part = rest.astype(B16)
        rest = rest - part.astype(F32)
        term = dot(part, b) if left else dot(a, part)
        total = term if total is None else total + term
    return total


def copy_to(src, dst, send, recv, device):
    return pltpu.make_async_remote_copy(
        src_ref=src,
        dst_ref=dst,
        send_sem=send,
        recv_sem=recv,
        device_id=device,
        device_id_type=pl.DeviceIdType.MESH,
    )


def kernel(
    tok, lengths, head_gain, mixer_gain, final_gain, rates,
    state_h, keys_h, values_h, wq_h, wk_h, wv_h, wg_h, wo_h, wu_h, wd_h,
    out,
    state, keys, values, factor, wp, wo, wu, wd, cosine, sine, offset,
    t_all, b1_out, b1_in0, b1_in1, b2_out, b2_in, retained, turned, heads, m_all, d_out, d_in,
    s_out, s_in, p_out, p_in, col_out, col_in, ends, lift, payload, hidden, h_all,
    g1_out, g1_in, g2_out, g2_in, g_sum, act_all, e_sum, e_out, e_in, j_out, j_in,
    local, send, r_w, r_a, r_b10, r_b11, r_b2, r_c, r_d, r_e, r_p, r_col, r_f, r_g1, r_g2, r_h1, r_h2, r_i, r_j,
):
    y, x, z, c = [lax.axis_index(name) for name in AXES]
    kv = y * 4 + x
    sibling = (y, x, z, 1 - c)
    row_of = lax.rem(x, 2)
    owner = row_of == c
    used = [0]
    pending = []

    def put(src, dst, recv, device, when=None):
        copy = copy_to(src, dst, send.at[used[0]], recv, device)
        used[0] += 1
        if when is None:
            copy.start()
        else:

            @pl.when(when)
            def _():
                copy.start()

        pending.append((when, copy))

    def settle():
        for when, copy in pending:
            if when is None:
                copy.wait_send()
            else:

                @pl.when(when)
                def _():
                    copy.wait_send()

        pending.clear()
        used[0] = 0

    def arrived(dst, sem, when=None):
        copy = copy_to(dst, dst, send.at[0], sem, sibling)
        if when is None:
            copy.wait_recv()
        else:

            @pl.when(when)
            def _():
                copy.wait_recv()

    here = []

    def fetch(src, dst):
        here.append(pltpu.make_async_copy(src, dst, local.at[len(here)]))
        here[-1].start()

    quarter = [wp.at[c, :, pl.ds(128 * i, 128)] for i in range(4)]
    for src, dst in zip((wq_h, wk_h, wv_h, wg_h), quarter):
        fetch(src, dst)
    fetch(wo_h, wo.at[c])
    fetch(wu_h, wu.at[c])
    fetch(wd_h, wd.at[c])
    fetch(keys_h, keys)
    fetch(values_h, values)
    fetch(state_h, state)

    barrier = pltpu.get_barrier_semaphore()
    greeted = 0
    for dy in range(4):
        for dx in range(4):
            for dc in range(2):
                if dy or dx or dc:
                    peer = (lax.rem(y + dy, 4), lax.rem(x + dx, 4), z, lax.rem(c + dc, 2))
                    pl.semaphore_signal(barrier, inc=1, device_id=peer, device_id_type=pl.DeviceIdType.MESH)
                    greeted += 1
    for dz in range(1, 8):
        peer = (y, x, lax.rem(z + dz, 8), c)
        pl.semaphore_signal(barrier, inc=1, device_id=peer, device_id_type=pl.DeviceIdType.MESH)
        greeted += 1

    ones = jnp.full((8, 256), 1.0, B16)
    first = jnp.where(lax.broadcasted_iota(jnp.int32, (8, 256), 0) == 0, 1.0, 0.0).astype(B16)
    lane = lax.broadcasted_iota(jnp.int32, (64, 128), 1)
    low = lax.rem(lane, HDIM) < HDIM // 2
    lane_row = lax.broadcasted_iota(jnp.int32, (1, 128), 1)
    rate = jnp.where(lane_row < HDIM, rates[0], rates[1])

    def row_sums(u):
        total = None
        for _ in range(3):
            part = u.astype(B16)
            u = u - part.astype(F32)
            term = lax.dot_general(ones, part, (((1,), (1,)), ((), ())), preferred_element_type=F32)
            total = term if total is None else total + term
        return total

    def column(u):
        total = None
        for _ in range(3):
            part = u.astype(B16)
            u = u - part.astype(F32)
            term = lax.dot_general(part, first, (((0,), (0,)), ((), ())), preferred_element_type=F32)
            total = term if total is None else total + term
        return total

    position = column(jnp.broadcast_to(lengths[...].astype(F32), (8, 64)))[:, :128]
    offset[...] = position - jnp.floor(position * (1.0 / BLK)) * BLK
    inverse = jnp.zeros((1, 128), F32)
    for i in range(HDIM // 2):
        inverse = jnp.where(lax.rem(lane_row, HDIM // 2) == i, 10000.0 ** (-i / (HDIM // 2)), inverse)
    angle = position * inverse
    cosine[...] = jnp.cos(angle)
    sines = jnp.sin(angle)
    sine[...] = jnp.where(low, -sines, sines)

    def decay(i, carry):
        rows = pl.ds(pl.multiple_of(i * 8, 8), 8)
        off = offset[rows, :][:, None, :]
        slot = lax.broadcasted_iota(jnp.int32, (8, BLK, 128), 1).astype(F32)
        lag = jnp.maximum(off - slot, 0.0)
        factor[rows] = jnp.where(slot < off, jnp.exp(-rate[None] * lag), 0.0)
        return carry

    lax.fori_loop(0, 8, decay, 0)
    t_all[z] = tok[...]
    pl.semaphore_wait(barrier, greeted)

    for d in NEAR[1:]:
        put(tok, t_all.at[z], r_a.at[z], (y, x, lax.rem(z + d, 8), c))
    for i, (src, dst) in enumerate(
        [*zip((wq_h, wk_h, wv_h, wg_h), quarter), (wo_h, wo.at[c]), (wu_h, wu.at[c]), (wd_h, wd.at[c])]
    ):
        put(src, dst, r_w.at[i], sibling)
    theirs = [wp.at[1 - c, :, pl.ds(128 * i, 128)] for i in range(4)] + [w.at[1 - c] for w in (wo, wu, wd)]
    for i in range(4):
        here[i].wait()
        arrived(theirs[i], r_w.at[i])

    for d in NEAR:
        zp = lax.rem(z + 8 - d, 8)
        if d:
            arrived(t_all.at[zp], r_a.at[zp])
        yd, side = zp // 2, lax.rem(zp, 2)
        xd = 2 * side + c
        rows = t_all[zp]
        for colour in range(2):
            part = dot(rows, wp[colour]).astype(B16)
            b1_out[zp, colour] = part
            if colour == 0:
                mine, dst, sem, to = xd == x, b1_in0.at[x, yd], r_b10.at[x, yd], (y, xd, z, c)
            else:
                mine, dst, sem, to = yd == y, b1_in1.at[y, side], r_b11.at[y, side], (yd, x, z, c)

            @pl.when(mine)
            def _():
                dst[...] = part

            put(b1_out.at[zp, colour], dst, sem, to, jnp.logical_not(mine))

    def first_stage_x(j):
        piece = lax.rem(z // 2 + j, 4)

        @pl.when(owner)
        def _():
            for k in (1, 3, 2):
                i = lax.rem(x + k, 4)
                arrived(b1_in0.at[i, piece], r_b10.at[i, piece])
            total = b1_in0[0, piece].astype(F32)
            for k in range(1, 4):
                total = total + b1_in0[k, piece].astype(F32)
            b2_out[j] = total.astype(B16)

        mine = jnp.logical_and(piece == y, c == 0)

        @pl.when(jnp.logical_and(owner, mine))
        def _():
            b2_in[y] = b2_out[j]

        put(
            b2_out.at[j], b2_in.at[y], r_b2.at[y], (piece, x, z, 0),
            jnp.logical_and(owner, jnp.logical_not(mine)),
        )

    def first_stage_y(j):
        side = lax.rem(z + j, 2)
        for k in (1, 3, 2):
            i = lax.rem(y + k, 4)
            arrived(b1_in1.at[i, side], r_b11.at[i, side])
        total = b1_in1[0, side].astype(F32)
        for k in range(1, 4):
            total = total + b1_in1[k, side].astype(F32)
        total = total.astype(B16)
        b2_out[4 + j] = total
        xd = 2 * side + c
        mine = jnp.logical_and(xd == x, c == 1)

        @pl.when(mine)
        def _():
            b2_in[x] = total

        put(b2_out.at[4 + j], b2_in.at[x], r_b2.at[x], (y, xd, z, 1), jnp.logical_not(mine))

    first_stage_x(0)
    first_stage_x(1)
    first_stage_y(0)
    first_stage_x(3)
    first_stage_y(1)
    first_stage_x(2)

    for i in (5, 6):
        here[i].wait()
        arrived(theirs[i], r_w.at[i])
    gain_rows = jnp.broadcast_to(mixer_gain[...], (8, 256))
    for half in range(2):
        col_out[:, pl.ds(1024 * half, 1024)] = split_dot(gain_rows, wu[half], 3)[0:1]
    col_in[kv] = col_out[...]
    for k in (5, 7, 13, 15, 6, 14, 9, 11, 10, 1, 4, 3, 12, 2, 8):
        to = (lax.rem(y + k // 4, 4), lax.rem(x + k % 4, 4), z, c)
        put(col_out, col_in.at[kv], r_col.at[kv], to)

    place_b2 = jnp.where(c == 0, y, x)
    for k in range(4):
        arrived(b2_in.at[k], r_b2.at[k], jnp.logical_not(jnp.logical_and(owner, place_b2 == k)))
    qkvg = b2_in[0].astype(F32)
    for k in range(1, 4):
        qkvg = qkvg + b2_in[k].astype(F32)

    row_id = lax.broadcasted_iota(jnp.int32, (128, 128), 0)
    col_id = lax.broadcasted_iota(jnp.int32, (128, 128), 1)
    same_head = jnp.where(row_id // HDIM == col_id // HDIM, 1.0, 0.0).astype(B16)

    def rotated(u):
        partner = jnp.where(low, pltpu.roll(u, 96, 1), pltpu.roll(u, 32, 1))
        return u * cosine[...] + partner * sine[...]

    query, keyed, valued, gated = [
        qkvg[:, 128 * i : 128 * (i + 1)].astype(B16).astype(F32) for i in range(4)
    ]
    q_rot = rotated(query).astype(B16).astype(F32)
    k_rot = (rotated(keyed) * 0.125).astype(B16).astype(F32)
    own = split_dot(q_rot * k_rot, same_head, 2).astype(B16).astype(F32)
    turned[...] = q_rot
    retained[...] = own * valued
    for copy in here[7:]:
        copy.wait()
    pick_lane = lax.broadcasted_iota(jnp.int32, (HDIM, 128), 1)
    pick_row = lax.broadcasted_iota(jnp.int32, (HDIM, 128), 0)
    pick = jnp.where(lax.rem(pick_lane, HDIM) == pick_row, 1.0, 0.0)

    def attend(i, carry):
        rows = pl.ds(pl.multiple_of(i * 8, 8), 8)
        q = turned[rows, :]
        products = (keys[rows].astype(F32) * q[:, None, :]).reshape(8 * BLK, 128)
        scores = split_dot(products, same_head, 2).reshape(8, BLK, 128)
        weights = (scores * factor[rows]).astype(B16).astype(F32)
        inner = jnp.sum(weights * values[rows].astype(F32), axis=1)
        spread = (q[:, None, :] * pick[None]).reshape(8 * HDIM, 128).astype(B16)
        wide = dot(spread, same_head).reshape(8, HDIM, 128)
        cross = jnp.sum(wide * state[rows], axis=1)
        carried = jnp.exp(-rate * (offset[rows, :] + 1.0))
        retained[rows, :] += inner + cross * carried
        return carry

    lax.fori_loop(0, 8, attend, 0)
    kept = retained[...]
    centred = kept - split_dot(kept, same_head, 3) * (1.0 / HDIM)
    variance = split_dot(centred * centred, same_head, 3) * (1.0 / HDIM)
    normed = centred * lax.rsqrt(variance + EPS) * head_gain[...]
    mixed = (gated / (1.0 + jnp.exp(-gated)) * normed).astype(B16)
    heads[...] = mixed
    half = kv // 2

    for k in (10, 5, 7, 13, 15, 6, 14, 9, 11, 1, 4, 3, 12, 2, 8, 0):
        to = (lax.rem(y + k // 4, 4), lax.rem(x + k % 4, 4), z, row_of)
        put(heads, m_all.at[half, c], r_c.at[half, c], to, None if k else jnp.logical_not(owner))

    @pl.when(owner)
    def _():
        m_all[half, c] = mixed

    here[4].wait()
    arrived(theirs[4], r_w.at[4])

    start = 2 * y + x // 2
    for j in (0, 1, 7, 2, 6, 3, 5, 4):
        i = lax.rem(start + j, 8)
        for core in range(2):
            arrived(
                m_all.at[i, core], r_c.at[i, core],
                jnp.logical_not(jnp.logical_and(2 * i + c == kv, c == core)),
            )
        part = (dot(m_all[i, 0], wo[0]) + dot(m_all[i, 1], wo[1])).astype(B16)
        mine = i == z

        @pl.when(mine)
        def _():
            d_in[i] = part

        d_out[i] = part
        put(d_out.at[i], d_in.at[z], r_d.at[z], (y, x, i, c), jnp.logical_not(mine))
    branch = d_in[z].astype(F32)
    for d in NEAR[1:]:
        i = lax.rem(z + 8 - d, 8)
        arrived(d_in.at[i], r_d.at[i])
        branch = branch + d_in[i].astype(F32)

    tall = ALPHA * tok[...].astype(F32) + branch
    part_mean = jnp.sum(tall, axis=1, keepdims=True) * (1.0 / 256)
    part_centred = tall - part_mean
    scaled = (part_centred * mixer_gain[...]).astype(B16)
    payload[...] = scaled
    h_all[z] = scaled
    for d in (4, 3, 5, 2, 6, 1, 7):
        put(payload, h_all.at[z], r_f.at[z], (y, x, lax.rem(z + d, 8), c))
    s_out[0] = row_sums(jnp.broadcast_to(part_mean, (64, 256))) * (1.0 / 256)
    s_out[1] = row_sums(part_centred * part_centred)
    s_in[kv] = s_out[...]
    for k in (10, 5, 7, 13, 15, 6, 14, 9, 11, 1, 4, 3, 12, 2, 8):
        to = (lax.rem(y + k // 4, 4), lax.rem(x + k % 4, 4), z, c)
        put(s_out, s_in.at[kv], r_e.at[kv], to)

    along = (x, y)

    def device_on(colour, stage, index):
        if (colour + stage) % 2 == 0:
            return (y, index, z, c)
        return (index, x, z, c)

    for d in NEAR:
        zp = lax.rem(z + 8 - d, 8)
        if d:
            arrived(h_all.at[zp], r_f.at[zp])
        yd, xd = zp // 2, lax.rem(zp, 2) * 2
        rows = h_all[zp]
        for colour in range(2):
            part = dot(rows, wu[colour]).astype(B16)
            for side in range(2):
                rows_of = part[32 * side : 32 * side + 32]
                me, to, piece = (x, xd + side, yd) if colour == 0 else (y, yd, xd + side)
                g1_out[colour, to, piece] = rows_of
                put(
                    g1_out.at[colour, to, piece], g1_in.at[colour, me, piece],
                    r_g1.at[colour, me, piece], device_on(colour, 0, to), to != me,
                )

    for k in (1, 4, 3, 12, 2, 8, 5, 7, 13, 15, 6, 14, 9, 11, 10):
        i = lax.rem(y + k // 4, 4) * 4 + lax.rem(x + k % 4, 4)
        arrived(s_in.at[i], r_e.at[i])
    means = s_in[:, 0]
    mean = jnp.sum(means, axis=0) * (1.0 / 16)
    shift = means - mean[None]
    spread = (jnp.sum(s_in[:, 1], axis=0) + 256.0 * jnp.sum(shift * shift, axis=0)) * (1.0 / 4096)
    scale = lax.rsqrt(spread + EPS)
    eight = lax.broadcasted_iota(jnp.int32, (8, 64), 0)
    for group in range(2):
        stacked = jnp.zeros((8, 64), F32)
        for k in range(8):
            stacked = jnp.where(eight == k, shift[8 * group + k], stacked)
        p_out[group] = stacked
    p_out[2] = scale
    mine = half == z

    @pl.when(mine)
    def _():
        p_in[...] = p_out[...]

    for d in range(1, 8):
        put(p_out, p_in, r_p.at[0], (y, x, lax.rem(z + d, 8), c), mine)
    own_shift = s_out[0] - mean
    hidden[...] = ((part_centred + column(own_shift)) * column(scale) * mixer_gain[...]).astype(B16)

    for k in range(1, 16):
        i = lax.rem(y + k // 4, 4) * 4 + lax.rem(x + k % 4, 4)
        arrived(col_in.at[i], r_col.at[i])
    wide_eight = lax.broadcasted_iota(jnp.int32, (8, 2048), 0)
    arrived(p_in, r_p.at[0], jnp.logical_not(mine))
    lifted = jnp.zeros((64, 2048), F32)
    for group in range(2):
        stacked = jnp.zeros((8, 2048), F32)
        for k in range(8):
            stacked = jnp.where(wide_eight == k, col_in[8 * group + k], stacked)
        shift_high = p_in[group].astype(B16)
        shift_low = (p_in[group] - shift_high.astype(F32)).astype(B16)
        col_high = stacked.astype(B16)
        col_low = (stacked - col_high.astype(F32)).astype(B16)
        for a, b in ((shift_high, col_high), (shift_high, col_low), (shift_low, col_high)):
            lifted = lifted + lax.dot_general(a, b, (((0,), (0,)), ((), ())), preferred_element_type=F32)
    upper = row_of == 1
    lift[...] = jnp.where(upper, lifted[32:], lifted[:32])
    scales = column(p_in[2])
    ends[...] = jnp.where(upper, scales[32:], scales[:32])

    for j in (0, 1, 3, 2):
        for colour in range(2):
            me, other = along[colour], along[1 - colour]
            piece = lax.rem(other + j, 4)
            total = g1_out[colour, me, piece].astype(F32)
            for d in (1, 3, 2):
                source = lax.rem(me + d, 4)
                arrived(g1_in.at[colour, source, piece], r_g1.at[colour, source, piece])
                total = total + g1_in[colour, source, piece].astype(F32)
            if j:
                g2_out[colour, piece] = total.astype(B16)
                put(
                    g2_out.at[colour, piece], g2_in.at[colour, other], r_g2.at[colour, other],
                    device_on(colour, 1, piece),
                )
            else:
                g_sum[colour] = total + lift[:, 1024 * colour : 1024 * colour + 1024]

    def place(colour, i, j):
        if colour == 0:
            return (colour, i, j)
        return (colour, j, i)

    for colour in range(2):
        me, other = along[colour], along[1 - colour]
        total = g_sum[colour]
        for d in (1, 3, 2):
            source = lax.rem(other + d, 4)
            arrived(g2_in.at[colour, source], r_g2.at[colour, source])
            total = total + g2_in[colour, source].astype(F32)
        times = jnp.concatenate([ends[...]] * 4, 1)
        active = jnp.square(jnp.maximum(total * times, 0.0)).astype(B16)
        spot = act_all.at[colour, y, x]
        act_all[colour, y, x] = active
        for d in (2, 1, 3):
            put(spot, spot, r_h1.at[colour, other], device_on(colour, 1, lax.rem(other + d, 4)))
        for d in (2, 1, 3):
            put(spot, spot, r_h2.at[colour, other, me], device_on(colour, 0, lax.rem(me + d, 4)))
    for j in (1, 3, 2):
        for colour in range(2):
            me, other = along[colour], along[1 - colour]
            source = lax.rem(other + j, 4)
            spot = act_all.at[place(colour, source, me)]
            arrived(spot, r_h1.at[colour, source])
            for d in (2, 1, 3):
                put(spot, spot, r_h2.at[colour, source, me], device_on(colour, 0, lax.rem(me + d, 4)))

    for j in (0, 1, 3, 2):
        for colour in range(2):
            me, other = along[colour], along[1 - colour]
            source = lax.rem(other + j, 4)
            for d in (1, 3, 2):
                at = lax.rem(me + d, 4)
                arrived(act_all.at[place(colour, source, at)], r_h2.at[colour, source, at])
            if colour == 0:
                rows = act_all[0, source].reshape(128, 1024)
            else:
                rows = act_all[1, :, source].reshape(128, 1024)
            e_sum[colour, source] = dot(rows, wd[colour]).reshape(4, 32, 256)
    for d in (4, 3, 5, 2, 6, 1, 7, 0):
        i = lax.rem(z + d, 8)
        yd, xd = i // 2, lax.rem(i, 2) * 2
        part = jnp.concatenate(
            [e_sum[0, yd, xd + side] + e_sum[1, xd + side, yd] for side in range(2)], 0
        )
        if d:
            e_out[i] = part.astype(B16)
            put(e_out.at[i], e_in.at[z], r_i.at[z], (y, x, i, c))
        else:
            downward = part
    for d in NEAR[1:]:
        i = lax.rem(z + 8 - d, 8)
        arrived(e_in.at[i], r_i.at[i])
        downward = downward + e_in[i].astype(F32)

    tall = ALPHA * hidden[...].astype(F32) + downward
    part_mean = jnp.sum(tall, axis=1, keepdims=True) * (1.0 / 256)
    part_centred = tall - part_mean
    j_out[0] = row_sums(jnp.broadcast_to(part_mean, (64, 256))) * (1.0 / 256)
    j_out[1] = row_sums(part_centred * part_centred)
    j_in[kv] = j_out[...]
    for k in (10, 5, 7, 13, 15, 6, 14, 9, 11, 1, 4, 3, 12, 2, 8):
        to = (lax.rem(y + k // 4, 4), lax.rem(x + k % 4, 4), z, c)
        put(j_out, j_in.at[kv], r_j.at[kv], to)
    for k in range(1, 16):
        i = lax.rem(y + k // 4, 4) * 4 + lax.rem(x + k % 4, 4)
        arrived(j_in.at[i], r_j.at[i])
    means = j_in[:, 0]
    mean = jnp.sum(means, axis=0) * (1.0 / 16)
    shift = means - mean[None]
    spread = (jnp.sum(j_in[:, 1], axis=0) + 256.0 * jnp.sum(shift * shift, axis=0)) * (1.0 / 4096)
    scale = lax.rsqrt(spread + EPS)
    out[...] = ((part_centred + column(j_out[0] - mean)) * column(scale) * final_gain[...]).astype(B16)
    settle()


def per_device(
    tokens, lengths, state_block, cached_keys, cached_values, query_weight, key_weight,
    value_weight, gate_weight, decay_rate, head_gain, out_weight, mixer_gain, up_weight,
    down_weight, final_gain,
):
    vmem = pl.BlockSpec(memory_space=pltpu.VMEM)
    smem = pl.BlockSpec(memory_space=pltpu.SMEM)
    anywhere = pl.BlockSpec(memory_space=pl.ANY)
    dma = pltpu.SemaphoreType.DMA
    scratch = [
        pltpu.VMEM((64, 64, 128), F32),
        pltpu.VMEM((64, 128, 128), B16),
        pltpu.VMEM((64, 128, 128), B16),
        pltpu.VMEM((64, 128, 128), F32),
        pltpu.VMEM((2, 256, 512), B16),
        pltpu.VMEM((2, 128, 256), B16),
        pltpu.VMEM((2, 256, 1024), B16),
        pltpu.VMEM((2, 1024, 256), B16),
        pltpu.VMEM((64, 128), F32),
        pltpu.VMEM((64, 128), F32),
        pltpu.VMEM((64, 128), F32),
        pltpu.VMEM((8, 64, 256), B16),
        pltpu.VMEM((8, 2, 64, 512), B16),
        pltpu.VMEM((4, 4, 64, 512), B16),
        pltpu.VMEM((4, 2, 64, 512), B16),
        pltpu.VMEM((6, 64, 512), B16),
        pltpu.VMEM((4, 64, 512), B16),
        pltpu.VMEM((64, 128), F32),
        pltpu.VMEM((64, 128), F32),
        pltpu.VMEM((64, 128), B16),
        pltpu.VMEM((8, 2, 64, 128), B16),
        pltpu.VMEM((8, 64, 256), B16),
        pltpu.VMEM((8, 64, 256), B16),
        pltpu.VMEM((2, 8, 64), F32),
        pltpu.VMEM((16, 2, 8, 64), F32),
        pltpu.VMEM((3, 8, 64), F32),
        pltpu.VMEM((3, 8, 64), F32),
        pltpu.VMEM((1, 2048), F32),
        pltpu.VMEM((16, 1, 2048), F32),
        pltpu.VMEM((32, 256), F32),
        pltpu.VMEM((32, 2048), F32),
        pltpu.VMEM((64, 256), B16),
        pltpu.VMEM((64, 256), B16),
        pltpu.VMEM((8, 64, 256), B16),
        pltpu.VMEM((2, 4, 4, 32, 1024), B16),
        pltpu.VMEM((2, 4, 4, 32, 1024), B16),
        pltpu.VMEM((2, 4, 32, 1024), B16),
        pltpu.VMEM((2, 4, 32, 1024), B16),
        pltpu.VMEM((2, 32, 1024), F32),
        pltpu.VMEM((2, 4, 4, 32, 1024), B16),
        pltpu.VMEM((2, 4, 4, 32, 256), F32),
        pltpu.VMEM((8, 64, 256), B16),
        pltpu.VMEM((8, 64, 256), B16),
        pltpu.VMEM((2, 8, 64), F32),
        pltpu.VMEM((16, 2, 8, 64), F32),
        dma((10,)),
        dma((200,)),
        dma((7,)),
        dma((8,)),
        dma((4, 4)),
        dma((4, 2)),
        dma((4,)),
        dma((8, 2)),
        dma((8,)),
        dma((16,)),
        dma((1,)),
        dma((16,)),
        dma((8,)),
        dma((2, 4, 4)),
        dma((2, 4)),
        dma((2, 4)),
        dma((2, 4, 4)),
        dma((8,)),
        dma((16,)),
    ]
    return pl.pallas_call(
        kernel,
        out_shape=jax.ShapeDtypeStruct((64, 256), B16),
        in_specs=[vmem] * 5 + [smem] + [anywhere] * 10,
        out_specs=vmem,
        scratch_shapes=scratch,
        name="layer",
        compiler_params=pltpu.CompilerParams(
            collective_id=0, has_side_effects=True, vmem_limit_bytes=56 * 1024 * 1024
        ),
    )(
        tokens, lengths[None, :], head_gain[None, :], mixer_gain[None, :], final_gain[None, :], decay_rate,
        state_block, cached_keys, cached_values, query_weight, key_weight, value_weight, gate_weight,
        out_weight, up_weight, down_weight,
    )


def solution(mesh):
    finer = Mesh(mesh.devices.reshape(4, 4, 8, 2), AXES)
    kv, tp = ("y", "x"), ("z", "c")
    placed = (
        P(tp, kv), P(kv), P(kv, None, tp), P(kv, None, tp), P(kv, None, tp),
        P(kv, tp), P(kv, tp), P(kv, tp), P(kv, tp), P(tp), P(tp), P(tp, kv), P(kv),
        P(kv, tp), P(tp, kv), P(kv),
    )
    return jax.shard_map(per_device, mesh=finer, in_specs=placed, out_specs=P(tp, kv), check_vma=False)
```

```python
import functools

import jax
import jax.numpy as jnp
from jax import lax
from jax.experimental import pallas as pl
from jax.experimental.pallas import tpu as pltpu
from jax.sharding import Mesh
from jax.sharding import PartitionSpec as P

HDIM = 64
BLK = 128
ALPHA = 2.0**0.5
EPS = 1e-05
AXES = ("y", "x", "z", "c")
NEAR = (0, 1, 7, 2, 6, 3, 5, 4)
F32 = jnp.float32
B16 = jnp.bfloat16


def dot(a, b):
    return jnp.dot(a, b, preferred_element_type=F32)


def split_dot(a, b, terms, left=True):
    total = None
    rest = a if left else b
    for _ in range(terms):
        part = rest.astype(B16)
        rest = rest - part.astype(F32)
        term = dot(part, b) if left else dot(a, part)
        total = term if total is None else total + term
    return total


def copy_to(src, dst, send, recv, device):
    return pltpu.make_async_remote_copy(
        src_ref=src,
        dst_ref=dst,
        send_sem=send,
        recv_sem=recv,
        device_id=device,
        device_id_type=pl.DeviceIdType.MESH,
    )


def kernel(
    tok, lengths, head_gain, mixer_gain, final_gain, rates,
    state_h, keys_h, values_h, wq_h, wk_h, wv_h, wg_h, wo_h, wu_h, wd_h,
    out,
    state, keys, values, factor, wp, wo, wu, wd, cosine, sine, offset,
    t_all, b1_out, b1_in0, b1_in1, b2_out, b2_in, retained, turned, heads, m_all, d_out, d_in,
    s_out, s_in, p_out, p_in, col_out, col_in, ends, lift, payload, hidden, h_all,
    g1_out, g1_inx, g1_iny, g2_out, g2_in, g_sum, act_all, e_out, e_in, j_out, j_in,
    local, send, r_w, r_a, r_b10, r_b11, r_b2, r_c, r_d, r_e, r_p, r_col, r_f,
    r_g1x, r_g1y, r_g2, r_h1, r_h2, r_i, r_j, r_x, r_v,
):
    y, x, z, c = [lax.axis_index(name) for name in AXES]
    kv = y * 4 + x
    sibling = (y, x, z, 1 - c)
    row_of = lax.rem(x, 2)
    owner = row_of == c
    pair = x // 2
    partner = (y, 2 * pair + 1 - row_of, z, c)
    used = [0]
    pending = []

    def put(src, dst, recv, device, when=None):
        copy = copy_to(src, dst, send.at[used[0]], recv, device)
        used[0] += 1
        if when is None:
            copy.start()
        else:

            @pl.when(when)
            def _():
                copy.start()

        pending.append((when, copy))

    def settle():
        for when, copy in pending:
            if when is None:
                copy.wait_send()
            else:

                @pl.when(when)
                def _():
                    copy.wait_send()

        pending.clear()
        used[0] = 0

    def arrived(dst, sem, when=None):
        copy = copy_to(dst, dst, send.at[0], sem, sibling)
        if when is None:
            copy.wait_recv()
        else:

            @pl.when(when)
            def _():
                copy.wait_recv()

    here = []

    def fetch(src, dst):
        here.append(pltpu.make_async_copy(src, dst, local.at[len(here)]))
        here[-1].start()

    quarter = [wp.at[c, :, pl.ds(128 * i, 128)] for i in range(4)]
    for src, dst in zip((wq_h, wk_h, wv_h, wg_h), quarter):
        fetch(src, dst)
    fetch(wo_h, wo.at[c])
    fetch(wu_h, wu.at[row_of, c])
    fetch(wd_h, wd.at[row_of, c])
    fetch(keys_h, keys)
    fetch(values_h, values)
    fetch(state_h, state)

    barrier = pltpu.get_barrier_semaphore()
    greeted = 0
    for dy in range(4):
        for dx in range(4):
            for dc in range(2):
                if dy or dx or dc:
                    peer = (lax.rem(y + dy, 4), lax.rem(x + dx, 4), z, lax.rem(c + dc, 2))
                    pl.semaphore_signal(barrier, inc=1, device_id=peer, device_id_type=pl.DeviceIdType.MESH)
                    greeted += 1
    for dz in range(1, 8):
        peer = (y, x, lax.rem(z + dz, 8), c)
        pl.semaphore_signal(barrier, inc=1, device_id=peer, device_id_type=pl.DeviceIdType.MESH)
        greeted += 1
        peer = (y, 2 * pair + 1 - row_of, lax.rem(z + dz, 8), c)
        pl.semaphore_signal(barrier, inc=1, device_id=peer, device_id_type=pl.DeviceIdType.MESH)
        greeted += 1

    ones = jnp.full((8, 256), 1.0, B16)
    first = jnp.where(lax.broadcasted_iota(jnp.int32, (8, 256), 0) == 0, 1.0, 0.0).astype(B16)
    lane = lax.broadcasted_iota(jnp.int32, (64, 128), 1)
    low = lax.rem(lane, HDIM) < HDIM // 2
    lane_row = lax.broadcasted_iota(jnp.int32, (1, 128), 1)
    rate = jnp.where(lane_row < HDIM, rates[0], rates[1])

    def row_sums(u):
        total = None
        for _ in range(3):
            part = u.astype(B16)
            u = u - part.astype(F32)
            term = lax.dot_general(ones, part, (((1,), (1,)), ((), ())), preferred_element_type=F32)
            total = term if total is None else total + term
        return total

    def packed_sums(part_mean, part_centred):
        means = jnp.broadcast_to(part_mean * (1.0 / 256), (64, 256))
        return row_sums(jnp.concatenate([means, part_centred * part_centred], 0))

    def combined(own_sums, sums):
        total = jnp.sum(sums[...], axis=0)
        mean = total * (1.0 / 16)
        shift = jnp.where((lane_row < 64)[None], sums[...] - mean[None], 0.0)
        between = jnp.sum(shift * shift, axis=0)
        spread = (pltpu.roll(total, 64, 1) + 256.0 * between) * (1.0 / 4096)
        scale = jnp.where(lane_row < 64, lax.rsqrt(spread + EPS), 0.0)
        own_shift = jnp.broadcast_to(jnp.where(lane_row < 64, own_sums[...] - mean, 0.0), (8, 128))
        return shift, own_shift, jnp.broadcast_to(scale, (8, 128))

    def column(u):
        total = None
        for _ in range(3):
            part = u.astype(B16)
            u = u - part.astype(F32)
            term = lax.dot_general(part, first, (((0,), (0,)), ((), ())), preferred_element_type=F32)
            total = term if total is None else total + term
        return total

    position = column(jnp.broadcast_to(lengths[...].astype(F32), (8, 64)))[:, :128]
    offset[...] = position - jnp.floor(position * (1.0 / BLK)) * BLK
    inverse = jnp.zeros((1, 128), F32)
    for i in range(HDIM // 2):
        inverse = jnp.where(lax.rem(lane_row, HDIM // 2) == i, 10000.0 ** (-i / (HDIM // 2)), inverse)
    angle = position * inverse
    cosine[...] = jnp.cos(angle)
    sines = jnp.sin(angle)
    sine[...] = jnp.where(low, -sines, sines)

    def decay(i, carry):
        rows = pl.ds(pl.multiple_of(i * 8, 8), 8)
        off = offset[rows, :][:, None, :]
        slot = lax.broadcasted_iota(jnp.int32, (8, BLK, 128), 1).astype(F32)
        lag = jnp.maximum(off - slot, 0.0)
        factor[rows] = jnp.where(slot < off, jnp.exp(-rate[None] * lag), 0.0)
        return carry

    lax.fori_loop(0, 8, decay, 0)
    t_all[z] = tok[...]
    pl.semaphore_wait(barrier, greeted)

    for d in NEAR[1:]:
        put(tok, t_all.at[z], r_a.at[z], (y, x, lax.rem(z + d, 8), c))
    for i, (src, dst) in enumerate(
        [*zip((wq_h, wk_h, wv_h, wg_h), quarter), (wo_h, wo.at[c])]
    ):
        put(src, dst, r_w.at[i], sibling)
    theirs = [wp.at[1 - c, :, pl.ds(128 * i, 128)] for i in range(4)]
    theirs += [wo.at[1 - c], wu.at[row_of, 1 - c], wd.at[row_of, 1 - c]]
    def chunk(k, side, core):
        if k < 2:
            return wu.at[side, core, pl.ds(128 * k, 128), :]
        return wd.at[side, core, pl.ds(512 * (k - 2), 512), :]

    def to_partner(k):
        put(chunk(k, row_of, c), chunk(k, row_of, c), r_x.at[k], partner)

    def on_to_sibling(k):
        arrived(chunk(k, 1 - row_of, c), r_x.at[k])
        put(chunk(k, 1 - row_of, c), chunk(k, 1 - row_of, c), r_v.at[k], sibling)

    here[5].wait()
    to_partner(0)
    for i in range(4):
        here[i].wait()
        arrived(theirs[i], r_w.at[i])

    for d in NEAR:
        zp = lax.rem(z + 8 - d, 8)
        if d:
            arrived(t_all.at[zp], r_a.at[zp])
        yd, side = zp // 2, lax.rem(zp, 2)
        xd = 2 * side + c
        rows = t_all[zp]
        for colour in range(2):
            part = dot(rows, wp[colour]).astype(B16)
            b1_out[zp, colour] = part
            if colour == 0:
                mine, dst, sem, to = xd == x, b1_in0.at[x, yd], r_b10.at[x, yd], (y, xd, z, c)
            else:
                mine, dst, sem, to = yd == y, b1_in1.at[y, side], r_b11.at[y, side], (yd, x, z, c)

            @pl.when(mine)
            def _():
                dst[...] = part

            put(b1_out.at[zp, colour], dst, sem, to, jnp.logical_not(mine))

    put(wu_h, wu.at[row_of, c], r_w.at[5], sibling)
    put(wd_h, wd.at[row_of, c], r_w.at[6], sibling)

    def first_stage_x(j):
        piece = lax.rem(z // 2 + j, 4)

        @pl.when(owner)
        def _():
            for k in (1, 3, 2):
                i = lax.rem(x + k, 4)
                arrived(b1_in0.at[i, piece], r_b10.at[i, piece])
            total = b1_in0[0, piece].astype(F32)
            for k in range(1, 4):
                total = total + b1_in0[k, piece].astype(F32)
            b2_out[j] = total.astype(B16)

        mine = jnp.logical_and(piece == y, c == 0)

        @pl.when(jnp.logical_and(owner, mine))
        def _():
            b2_in[y] = b2_out[j]

        put(
            b2_out.at[j], b2_in.at[y], r_b2.at[y], (piece, x, z, 0),
            jnp.logical_and(owner, jnp.logical_not(mine)),
        )

    def first_stage_y(j):
        side = lax.rem(z + j, 2)
        for k in (1, 3, 2):
            i = lax.rem(y + k, 4)
            arrived(b1_in1.at[i, side], r_b11.at[i, side])
        total = b1_in1[0, side].astype(F32)
        for k in range(1, 4):
            total = total + b1_in1[k, side].astype(F32)
        total = total.astype(B16)
        b2_out[4 + j] = total
        xd = 2 * side + c
        mine = jnp.logical_and(xd == x, c == 1)

        @pl.when(mine)
        def _():
            b2_in[x] = total

        put(b2_out.at[4 + j], b2_in.at[x], r_b2.at[x], (y, xd, z, 1), jnp.logical_not(mine))

    first_stage_x(0)
    first_stage_x(1)
    first_stage_y(0)
    first_stage_x(3)
    first_stage_y(1)
    first_stage_x(2)

    here[6].wait()
    to_partner(1)
    for i in (5, 6):
        arrived(theirs[i], r_w.at[i])
    gain_rows = jnp.broadcast_to(mixer_gain[...], (8, 256))
    for half in range(2):
        col_out[:, pl.ds(1024 * half, 1024)] = split_dot(gain_rows, wu[row_of, half], 3)[0:1]
    col_in[kv] = col_out[...]
    for k in (5, 7, 13, 15, 6, 14, 9, 11, 10, 1, 4, 3, 12, 2, 8):
        to = (lax.rem(y + k // 4, 4), lax.rem(x + k % 4, 4), z, c)
        put(col_out, col_in.at[kv], r_col.at[kv], to)

    place_b2 = jnp.where(c == 0, y, x)
    for k in range(4):
        arrived(b2_in.at[k], r_b2.at[k], jnp.logical_not(jnp.logical_and(owner, place_b2 == k)))
    qkvg = b2_in[0].astype(F32)
    for k in range(1, 4):
        qkvg = qkvg + b2_in[k].astype(F32)

    row_id = lax.broadcasted_iota(jnp.int32, (128, 128), 0)
    col_id = lax.broadcasted_iota(jnp.int32, (128, 128), 1)
    same_head = jnp.where(row_id // HDIM == col_id // HDIM, 1.0, 0.0).astype(B16)

    def rotated(u):
        partner = jnp.where(low, pltpu.roll(u, 96, 1), pltpu.roll(u, 32, 1))
        return u * cosine[...] + partner * sine[...]

    query, keyed, valued, gated = [
        qkvg[:, 128 * i : 128 * (i + 1)].astype(B16).astype(F32) for i in range(4)
    ]
    q_rot = rotated(query).astype(B16).astype(F32)
    k_rot = (rotated(keyed) * 0.125).astype(B16).astype(F32)
    own = split_dot(q_rot * k_rot, same_head, 2).astype(B16).astype(F32)
    turned[...] = q_rot
    retained[...] = own * valued
    for copy in here[7:]:
        copy.wait()
    pick_lane = lax.broadcasted_iota(jnp.int32, (HDIM, 128), 1)
    pick_row = lax.broadcasted_iota(jnp.int32, (HDIM, 128), 0)
    pick = jnp.where(lax.rem(pick_lane, HDIM) == pick_row, 1.0, 0.0)

    def attend(i, carry):
        rows = pl.ds(pl.multiple_of(i * 8, 8), 8)
        q = turned[rows, :]
        products = (keys[rows] * q.astype(B16)[:, None, :]).reshape(8 * BLK, 128)
        scores = dot(products, same_head).reshape(8, BLK, 128)
        weights = (scores * factor[rows]).astype(B16).astype(F32)
        inner = jnp.sum(weights * values[rows].astype(F32), axis=1)
        spread = (q[:, None, :] * pick[None]).reshape(8 * HDIM, 128).astype(B16)
        wide = dot(spread, same_head).reshape(8, HDIM, 128)
        cross = jnp.sum(wide * state[rows], axis=1)
        carried = jnp.exp(-rate * (offset[rows, :] + 1.0))
        retained[rows, :] += inner + cross * carried
        return carry

    lax.fori_loop(0, 8, attend, 0)
    kept = retained[...]
    centred = kept - split_dot(kept, same_head, 3) * (1.0 / HDIM)
    variance = split_dot(centred * centred, same_head, 3) * (1.0 / HDIM)
    normed = centred * lax.rsqrt(variance + EPS) * head_gain[...]
    mixed = (gated / (1.0 + jnp.exp(-gated)) * normed).astype(B16)
    heads[...] = mixed
    half = kv // 2

    for k in (10, 5, 7, 13, 15, 6, 14, 9, 11, 1, 4, 3, 12, 2, 8, 0):
        to = (lax.rem(y + k // 4, 4), lax.rem(x + k % 4, 4), z, row_of)
        put(heads, m_all.at[half, c], r_c.at[half, c], to, None if k else jnp.logical_not(owner))

    @pl.when(owner)
    def _():
        m_all[half, c] = mixed

    for k in range(2, 4):
        to_partner(k)
    on_to_sibling(0)

    here[4].wait()
    arrived(theirs[4], r_w.at[4])

    start = 2 * y + x // 2
    for j in (0, 1, 7, 2, 6, 3, 5, 4):
        i = lax.rem(start + j, 8)
        for core in range(2):
            arrived(
                m_all.at[i, core], r_c.at[i, core],
                jnp.logical_not(jnp.logical_and(2 * i + c == kv, c == core)),
            )
        part = (dot(m_all[i, 0], wo[0]) + dot(m_all[i, 1], wo[1])).astype(B16)
        mine = i == z

        @pl.when(mine)
        def _():
            d_in[i] = part

        d_out[i] = part
        put(d_out.at[i], d_in.at[z], r_d.at[z], (y, x, i, c), jnp.logical_not(mine))
    on_to_sibling(1)
    branch = d_in[z].astype(F32)
    for d in NEAR[1:]:
        i = lax.rem(z + 8 - d, 8)
        arrived(d_in.at[i], r_d.at[i])
        branch = branch + d_in[i].astype(F32)

    tall = ALPHA * tok[...].astype(F32) + branch
    part_mean = jnp.sum(tall, axis=1, keepdims=True) * (1.0 / 256)
    part_centred = tall - part_mean
    scaled = (part_centred * mixer_gain[...]).astype(B16)
    payload[...] = scaled
    turn = lax.rem(z, 2)
    stays = turn == row_of

    @pl.when(stays)
    def _():
        h_all[z // 2, row_of] = scaled

    for d in (4, 3, 5, 2, 6, 1, 7, 0):
        put(
            payload, h_all.at[z // 2, row_of], r_f.at[z // 2, row_of],
            (y, 2 * pair + turn, lax.rem(z + d, 8), c), None if d else jnp.logical_not(stays),
        )
    s_out[...] = packed_sums(part_mean, part_centred)[0:1]
    s_in[kv] = s_out[...]
    for k in (10, 5, 7, 13, 15, 6, 14, 9, 11, 1, 4, 3, 12, 2, 8):
        to = (lax.rem(y + k // 4, 4), lax.rem(x + k % 4, 4), z, c)
        put(s_out, s_in.at[kv], r_e.at[kv], to)

    for k in range(2):
        arrived(chunk(k, 1 - row_of, 1 - c), r_v.at[k])

    along = (pair, y)
    size = (2, 4)

    def device_on(colour, stage, index):
        if (colour + stage) % 2 == 0:
            return (y, 2 * index + row_of, z, c)
        return (index, x, z, c)

    for d in range(4):
        t = lax.rem(z // 2 + (0, 1, 3, 2)[d], 4)
        for side in range(2):
            here_already = jnp.logical_and(2 * t + row_of == z, row_of == side)
            arrived(h_all.at[t, side], r_f.at[t, side], jnp.logical_not(here_already))
        for colour in range(2):
            part = (dot(h_all[t, 0], wu[0, colour]) + dot(h_all[t, 1], wu[1, colour])).astype(B16)
            for side in range(2):
                g1_out[colour, t, side] = part[32 * side : 32 * side + 32]
                spot = g1_out.at[colour, t, side]
                if colour == 0:
                    put(
                        spot, g1_inx.at[pair, t], r_g1x.at[pair, t], device_on(0, 0, side),
                        pair != side,
                    )
                else:
                    put(spot, g1_iny.at[y, side], r_g1y.at[y, side], device_on(1, 0, t), y != t)

    for k in (1, 4, 3, 12, 2, 8, 5, 7, 13, 15, 6, 14, 9, 11, 10):
        i = lax.rem(y + k // 4, 4) * 4 + lax.rem(x + k % 4, 4)
        arrived(s_in.at[i], r_e.at[i])
    shift, own_shift, scale = combined(s_out, s_in)
    eight = lax.broadcasted_iota(jnp.int32, (8, 128), 0)
    for group in range(2):
        stacked = jnp.zeros((8, 128), F32)
        for k in range(8):
            stacked = jnp.where(eight == k, shift[8 * group + k], stacked)
        p_out[group] = stacked
    p_out[2] = scale
    ends_at = 2 * y + row_of
    mine = ends_at == z

    @pl.when(mine)
    def _():
        p_in[...] = p_out[...]

    for d in range(1, 8):
        put(p_out, p_in, r_p.at[0], (y, x, lax.rem(z + d, 8), c), mine)
    wide_shift, wide_scale = column(own_shift)[:64], column(scale)[:64]
    hidden[...] = ((part_centred + wide_shift) * wide_scale * mixer_gain[...]).astype(B16)

    def first_sum(colour, j):
        me, other = along[colour], along[1 - colour]
        piece = lax.rem(other + j, size[1 - colour])
        total = (g1_out[0, piece, me] if colour == 0 else g1_out[1, me, piece]).astype(F32)
        for d in (1, 3, 2) if colour else (1,):
            source = lax.rem(me + d, size[colour])
            spot, sem = (g1_iny, r_g1y) if colour else (g1_inx, r_g1x)
            arrived(spot.at[source, piece], sem.at[source, piece])
            total = total + spot[source, piece].astype(F32)
        if j:
            g2_out[colour, piece] = total.astype(B16)
            put(
                g2_out.at[colour, piece], g2_in.at[colour, other], r_g2.at[colour, other],
                device_on(colour, 1, piece),
            )
        else:
            g_sum[colour] = total + lift[:, 1024 * colour : 1024 * colour + 1024]

    for colour, j in ((0, 2), (1, 1), (0, 1), (0, 3)):
        first_sum(colour, j)

    for k in range(1, 16):
        i = lax.rem(y + k // 4, 4) * 4 + lax.rem(x + k % 4, 4)
        arrived(col_in.at[i], r_col.at[i])
    wide_eight = lax.broadcasted_iota(jnp.int32, (8, 2048), 0)
    arrived(p_in, r_p.at[0], jnp.logical_not(mine))
    lifted = jnp.zeros((128, 2048), F32)
    for group in range(2):
        stacked = jnp.zeros((8, 2048), F32)
        for k in range(8):
            stacked = jnp.where(wide_eight == k, col_in[8 * group + k], stacked)
        shift_high = p_in[group].astype(B16)
        shift_low = (p_in[group] - shift_high.astype(F32)).astype(B16)
        col_high = stacked.astype(B16)
        col_low = (stacked - col_high.astype(F32)).astype(B16)
        for a, b in ((shift_high, col_high), (shift_high, col_low), (shift_low, col_high)):
            lifted = lifted + lax.dot_general(a, b, (((0,), (0,)), ((), ())), preferred_element_type=F32)
    upper = pair == 1
    lift[...] = jnp.where(upper, lifted[32:64], lifted[:32])
    scales = column(p_in[2])
    ends[...] = jnp.where(upper, scales[32:64], scales[:32])

    for colour, j in ((0, 0), (1, 0)):
        first_sum(colour, j)
    for k in range(2, 4):
        on_to_sibling(k)

    def others(n):
        return (2, 1, 3) if n == 4 else (1,)

    for colour in range(2):
        me, other = along[colour], along[1 - colour]
        total = g_sum[colour]
        for d in others(size[1 - colour]):
            source = lax.rem(other + d, size[1 - colour])
            arrived(g2_in.at[colour, source], r_g2.at[colour, source])
            total = total + g2_in[colour, source].astype(F32)
        times = jnp.concatenate([ends[...]] * 4, 1)
        active = jnp.square(jnp.maximum(total * times, 0.0)).astype(B16)
        spot = act_all.at[colour, y, pair]
        act_all[colour, y, pair] = active
        for stage in (1, 0):
            at = along[colour] if stage == 0 else along[1 - colour]
            n = size[(colour + stage) % 2]
            sem = r_h2.at[colour, y, pair] if stage == 0 else r_h1.at[colour, other]
            for d in others(n):
                put(spot, spot, sem, device_on(colour, stage, lax.rem(at + d, n)))

    def forward(colour, j):
        me, other = along[colour], along[1 - colour]
        source = lax.rem(other + j, size[1 - colour])
        where = (source, pair) if colour == 0 else (y, source)
        spot = act_all.at[colour, where[0], where[1]]
        arrived(spot, r_h1.at[colour, source])
        for d in others(size[colour]):
            put(
                spot, spot, r_h2.at[colour, where[0], where[1]],
                device_on(colour, 0, lax.rem(me + d, size[colour])),
            )

    for colour, j in ((1, 1), (0, 1), (0, 3), (0, 2)):
        forward(colour, j)

    for k in range(2, 4):
        arrived(chunk(k, 1 - row_of, 1 - c), r_v.at[k])

    for j in (0, 1, 3, 2):
        t = lax.rem(y + j, 4)
        for colour in range(2):
            for side in range(2):
                if colour == 0:
                    arrived(act_all.at[0, t, side], r_h2.at[0, t, side], pair != side)
                elif j:
                    arrived(act_all.at[1, t, side], r_h2.at[1, t, side])
        upper_rows = act_all[0, t].reshape(64, 1024)
        lower_rows = act_all[1, t].reshape(64, 1024)
        for side in range(2):
            part = (dot(upper_rows, wd[side, 0]) + dot(lower_rows, wd[side, 1])).astype(B16)
            keep = jnp.logical_and(2 * t + row_of == z, row_of == side)
            e_out[t, side] = part

            @pl.when(keep)
            def _():
                e_in[z] = part

            put(
                e_out.at[t, side], e_in.at[z], r_i.at[z], (y, 2 * pair + side, 2 * t + row_of, c),
                jnp.logical_not(keep),
            )
    downward = None
    for d in NEAR:
        i = lax.rem(z + 8 - d, 8)
        arrived(e_in.at[i], r_i.at[i], None if d else jnp.logical_not(stays))
        term = e_in[i].astype(F32)
        downward = term if downward is None else downward + term

    tall = ALPHA * hidden[...].astype(F32) + downward
    part_mean = jnp.sum(tall, axis=1, keepdims=True) * (1.0 / 256)
    part_centred = tall - part_mean
    j_out[...] = packed_sums(part_mean, part_centred)[0:1]
    j_in[kv] = j_out[...]
    for k in (10, 5, 7, 13, 15, 6, 14, 9, 11, 1, 4, 3, 12, 2, 8):
        to = (lax.rem(y + k // 4, 4), lax.rem(x + k % 4, 4), z, c)
        put(j_out, j_in.at[kv], r_j.at[kv], to)
    for k in range(1, 16):
        i = lax.rem(y + k // 4, 4) * 4 + lax.rem(x + k % 4, 4)
        arrived(j_in.at[i], r_j.at[i])
    shift, own_shift, scale = combined(j_out, j_in)
    wide_shift, wide_scale = column(own_shift)[:64], column(scale)[:64]
    out[...] = ((part_centred + wide_shift) * wide_scale * final_gain[...]).astype(B16)
    settle()


def per_device(
    tokens, lengths, state_block, cached_keys, cached_values, query_weight, key_weight,
    value_weight, gate_weight, decay_rate, head_gain, out_weight, mixer_gain, up_weight,
    down_weight, final_gain,
):
    vmem = pl.BlockSpec(memory_space=pltpu.VMEM)
    smem = pl.BlockSpec(memory_space=pltpu.SMEM)
    anywhere = pl.BlockSpec(memory_space=pl.ANY)
    dma = pltpu.SemaphoreType.DMA
    scratch = [
        pltpu.VMEM((64, 64, 128), F32),
        pltpu.VMEM((64, 128, 128), B16),
        pltpu.VMEM((64, 128, 128), B16),
        pltpu.VMEM((64, 128, 128), F32),
        pltpu.VMEM((2, 256, 512), B16),
        pltpu.VMEM((2, 128, 256), B16),
        pltpu.VMEM((2, 2, 256, 1024), B16),
        pltpu.VMEM((2, 2, 1024, 256), B16),
        pltpu.VMEM((64, 128), F32),
        pltpu.VMEM((64, 128), F32),
        pltpu.VMEM((64, 128), F32),
        pltpu.VMEM((8, 64, 256), B16),
        pltpu.VMEM((8, 2, 64, 512), B16),
        pltpu.VMEM((4, 4, 64, 512), B16),
        pltpu.VMEM((4, 2, 64, 512), B16),
        pltpu.VMEM((6, 64, 512), B16),
        pltpu.VMEM((4, 64, 512), B16),
        pltpu.VMEM((64, 128), F32),
        pltpu.VMEM((64, 128), F32),
        pltpu.VMEM((64, 128), B16),
        pltpu.VMEM((8, 2, 64, 128), B16),
        pltpu.VMEM((8, 64, 256), B16),
        pltpu.VMEM((8, 64, 256), B16),
        pltpu.VMEM((1, 128), F32),
        pltpu.VMEM((16, 1, 128), F32),
        pltpu.VMEM((3, 8, 128), F32),
        pltpu.VMEM((3, 8, 128), F32),
        pltpu.VMEM((1, 2048), F32),
        pltpu.VMEM((16, 1, 2048), F32),
        pltpu.VMEM((32, 256), F32),
        pltpu.VMEM((32, 2048), F32),
        pltpu.VMEM((64, 256), B16),
        pltpu.VMEM((64, 256), B16),
        pltpu.VMEM((4, 2, 64, 256), B16),
        pltpu.VMEM((2, 4, 2, 32, 1024), B16),
        pltpu.VMEM((2, 4, 32, 1024), B16),
        pltpu.VMEM((4, 2, 32, 1024), B16),
        pltpu.VMEM((2, 4, 32, 1024), B16),
        pltpu.VMEM((2, 4, 32, 1024), B16),
        pltpu.VMEM((2, 32, 1024), F32),
        pltpu.VMEM((2, 4, 2, 32, 1024), B16),
        pltpu.VMEM((4, 2, 64, 256), B16),
        pltpu.VMEM((8, 64, 256), B16),
        pltpu.VMEM((1, 128), F32),
        pltpu.VMEM((16, 1, 128), F32),
        dma((10,)),
        dma((200,)),
        dma((7,)),
        dma((8,)),
        dma((4, 4)),
        dma((4, 2)),
        dma((4,)),
        dma((8, 2)),
        dma((8,)),
        dma((16,)),
        dma((1,)),
        dma((16,)),
        dma((4, 2)),
        dma((2, 4)),
        dma((4, 2)),
        dma((2, 4)),
        dma((2, 4)),
        dma((2, 4, 2)),
        dma((8,)),
        dma((16,)),
        dma((4,)),
        dma((4,)),
    ]
    return pl.pallas_call(
        kernel,
        out_shape=jax.ShapeDtypeStruct((64, 256), B16),
        in_specs=[vmem] * 5 + [smem] + [anywhere] * 10,
        out_specs=vmem,
        scratch_shapes=scratch,
        name="layer",
        compiler_params=pltpu.CompilerParams(
            collective_id=0, has_side_effects=True, vmem_limit_bytes=56 * 1024 * 1024
        ),
    )(
        tokens, lengths[None, :], head_gain[None, :], mixer_gain[None, :], final_gain[None, :], decay_rate,
        state_block, cached_keys, cached_values, query_weight, key_weight, value_weight, gate_weight,
        out_weight, up_weight, down_weight,
    )


def solution(mesh):
    finer = Mesh(mesh.devices.reshape(4, 4, 8, 2), AXES)
    kv, tp = ("y", "x"), ("z", "c")
    placed = (
        P(tp, kv), P(kv), P(kv, None, tp), P(kv, None, tp), P(kv, None, tp),
        P(kv, tp), P(kv, tp), P(kv, tp), P(kv, tp), P(tp), P(tp), P(tp, kv), P(kv),
        P(kv, tp), P(tp, kv), P(kv),
    )
    return jax.shard_map(per_device, mesh=finer, in_specs=placed, out_specs=P(tp, kv), check_vma=False)
```

```python
import functools

import jax
import jax.numpy as jnp
from jax import lax
from jax.experimental import pallas as pl
from jax.experimental.pallas import tpu as pltpu
from jax.sharding import Mesh
from jax.sharding import PartitionSpec as P

HDIM = 64
BLK = 128
ALPHA = 2.0**0.5
EPS = 1e-05
AXES = ("y", "x", "z", "c")
NEAR = (0, 1, 7, 2, 6, 3, 5, 4)
POOL = 32
SENDS = 36
F32 = jnp.float32
B16 = jnp.bfloat16


def dot(a, b):
    return jnp.dot(a, b, preferred_element_type=F32)


def split_dot(a, b, terms, left=True):
    total = None
    rest = a if left else b
    for _ in range(terms):
        part = rest.astype(B16)
        rest = rest - part.astype(F32)
        term = dot(part, b) if left else dot(a, part)
        total = term if total is None else total + term
    return total


def copy_to(src, dst, send, recv, device):
    return pltpu.make_async_remote_copy(
        src_ref=src,
        dst_ref=dst,
        send_sem=send,
        recv_sem=recv,
        device_id=device,
        device_id_type=pl.DeviceIdType.MESH,
    )


def kernel(
    tok_h, lengths_h, head_gain_h, mixer_gain_h, final_gain_h, rates,
    state_h, keys_h, values_h, wq_h, wk_h, wv_h, wg_h, wo_h, wu_h, wd_h,
    out,
    tok, lengths, head_gain, mixer_gain, final_gain, state, keys, values, factor, wp, wo, wu, wd, cosine, sine, offset,
    t_all, b1_out, b1_in0, b1_in1, b2_out, b2_in, retained, turned, heads, m_all, d_out, d_in,
    s_out, s_in, p_out, p_in, col_out, col_in, ends, lift, payload, hidden, h_all,
    g1_out, g1_inx, g1_iny, g2_out, g2_in, g_sum, act_all, e_out, e_in, j_out, j_in,
    local, send, r_w, r_a, r_b10, r_b11, r_b2, r_c, r_d, r_e, r_p, r_col, r_f,
    r_g1x, r_g1y, r_g2, r_h1, r_h2, r_i, r_j, r_x, r_v,
):
    y, x, z, c = [lax.axis_index(name) for name in AXES]
    kv = y * 4 + x
    sibling = (y, x, z, 1 - c)
    row_of = lax.rem(x, 2)
    owner = row_of == c
    pair = x // 2
    partner = (y, 2 * pair + 1 - row_of, z, c)
    pending = [None] * SENDS
    used = [0]

    def sent(slot):
        if pending[slot] is None:
            return
        when, copy = pending[slot]
        pending[slot] = None
        if when is None:
            copy.wait_send()
        else:

            @pl.when(when)
            def _():
                copy.wait_send()

    def put(src, dst, recv, device, when=None, slot=None):
        if slot is None:
            slot = used[0] % POOL
            used[0] += 1
        sent(slot)
        copy = copy_to(src, dst, send.at[slot], recv, device)
        if when is None:
            copy.start()
        else:

            @pl.when(when)
            def _():
                copy.start()

        pending[slot] = (when, copy)

    def settle():
        for slot in range(SENDS):
            sent(slot)

    def arrived(dst, sem, when=None):
        copy = copy_to(dst, dst, send.at[0], sem, sibling)
        if when is None:
            copy.wait_recv()
        else:

            @pl.when(when)
            def _():
                copy.wait_recv()

    barrier = pltpu.get_barrier_semaphore()
    greeted = 0
    for dy in range(4):
        for dx in range(4):
            for dc in range(2):
                if dy or dx or dc:
                    peer = (lax.rem(y + dy, 4), lax.rem(x + dx, 4), z, lax.rem(c + dc, 2))
                    pl.semaphore_signal(barrier, inc=1, device_id=peer, device_id_type=pl.DeviceIdType.MESH)
                    greeted += 1
    for dz in range(1, 8):
        peer = (y, x, lax.rem(z + dz, 8), c)
        pl.semaphore_signal(barrier, inc=1, device_id=peer, device_id_type=pl.DeviceIdType.MESH)
        greeted += 1
        peer = (y, 2 * pair + 1 - row_of, lax.rem(z + dz, 8), c)
        pl.semaphore_signal(barrier, inc=1, device_id=peer, device_id_type=pl.DeviceIdType.MESH)
        greeted += 1

    small = []
    for src, dst in (
        (lengths_h, lengths), (tok_h, tok), (head_gain_h, head_gain), (mixer_gain_h, mixer_gain),
        (final_gain_h, final_gain),
    ):
        small.append(pltpu.make_async_copy(src, dst, local.at[10 + len(small)]))
        small[-1].start()

    here = []

    def fetch(src, dst):
        here.append(pltpu.make_async_copy(src, dst, local.at[len(here)]))
        here[-1].start()

    quarter = [wp.at[c, :, pl.ds(128 * i, 128)] for i in range(4)]
    for src, dst in zip((wq_h, wk_h, wv_h, wg_h), quarter):
        fetch(src, dst)
    fetch(wo_h, wo.at[c])
    fetch(wu_h, wu.at[row_of, c])
    fetch(wd_h, wd.at[row_of, c])
    fetch(keys_h, keys)
    fetch(values_h, values)
    fetch(state_h, state)

    ones = jnp.full((8, 256), 1.0, B16)
    first = jnp.where(lax.broadcasted_iota(jnp.int32, (8, 256), 0) == 0, 1.0, 0.0).astype(B16)
    lane = lax.broadcasted_iota(jnp.int32, (64, 128), 1)
    low = lax.rem(lane, HDIM) < HDIM // 2
    lane_row = lax.broadcasted_iota(jnp.int32, (1, 128), 1)
    rate = jnp.where(lane_row < HDIM, rates[0], rates[1])

    def row_sums(u):
        total = None
        for _ in range(3):
            part = u.astype(B16)
            u = u - part.astype(F32)
            term = lax.dot_general(ones, part, (((1,), (1,)), ((), ())), preferred_element_type=F32)
            total = term if total is None else total + term
        return total

    def packed_sums(part_mean, part_centred):
        means = jnp.broadcast_to(part_mean * (1.0 / 256), (64, 256))
        return row_sums(jnp.concatenate([means, part_centred * part_centred], 0))

    def combined(own_sums, sums):
        total = jnp.sum(sums[...], axis=0)
        mean = total * (1.0 / 16)
        shift = jnp.where((lane_row < 64)[None], sums[...] - mean[None], 0.0)
        between = jnp.sum(shift * shift, axis=0)
        spread = (pltpu.roll(total, 64, 1) + 256.0 * between) * (1.0 / 4096)
        scale = jnp.where(lane_row < 64, lax.rsqrt(spread + EPS), 0.0)
        own_shift = jnp.broadcast_to(jnp.where(lane_row < 64, own_sums[...] - mean, 0.0), (8, 128))
        return shift, own_shift, jnp.broadcast_to(scale, (8, 128))

    def column(u):
        total = None
        for _ in range(3):
            part = u.astype(B16)
            u = u - part.astype(F32)
            term = lax.dot_general(part, first, (((0,), (0,)), ((), ())), preferred_element_type=F32)
            total = term if total is None else total + term
        return total

    small[0].wait()
    position = column(jnp.broadcast_to(lengths[...].astype(F32), (8, 64)))[:, :128]
    offset[...] = position - jnp.floor(position * (1.0 / BLK)) * BLK
    inverse = jnp.zeros((1, 128), F32)
    for i in range(HDIM // 2):
        inverse = jnp.where(lax.rem(lane_row, HDIM // 2) == i, 10000.0 ** (-i / (HDIM // 2)), inverse)
    angle = position * inverse
    cosine[...] = jnp.cos(angle)
    sines = jnp.sin(angle)
    sine[...] = jnp.where(low, -sines, sines)

    def decay(i, carry):
        rows = pl.ds(pl.multiple_of(i * 8, 8), 8)
        off = offset[rows, :][:, None, :]
        slot = lax.broadcasted_iota(jnp.int32, (8, BLK, 128), 1).astype(F32)
        lag = jnp.maximum(off - slot, 0.0)
        factor[rows] = jnp.where(slot < off, jnp.exp(-rate[None] * lag), 0.0)
        return carry

    lax.fori_loop(0, 8, decay, 0)
    for copy in small[1:]:
        copy.wait()
    t_all[z] = tok[...]
    pl.semaphore_wait(barrier, greeted)

    for d in NEAR[1:]:
        put(tok, t_all.at[z], r_a.at[z], (y, x, lax.rem(z + d, 8), c))
    for i, (src, dst) in enumerate(
        [*zip((wq_h, wk_h, wv_h, wg_h), quarter), (wo_h, wo.at[c])]
    ):
        put(src, dst, r_w.at[max(i - 3, 0)], sibling)
    theirs = [wp.at[1 - c], wo.at[1 - c], wu.at[row_of, 1 - c], wd.at[row_of, 1 - c]]
    def chunk(k, side, core):
        if k < 2:
            return wu.at[side, core, pl.ds(128 * k, 128), :]
        return wd.at[side, core, pl.ds(512 * (k - 2), 512), :]

    def to_partner(k):
        put(chunk(k, row_of, c), chunk(k, row_of, c), r_x.at[k], partner, slot=POOL + k)

    def on_to_sibling(k):
        arrived(chunk(k, 1 - row_of, c), r_x.at[k])
        put(chunk(k, 1 - row_of, c), chunk(k, 1 - row_of, c), r_v.at[k], sibling)

    here[5].wait()
    to_partner(0)
    for i in range(4):
        here[i].wait()
    arrived(theirs[0], r_w.at[0])

    for d in NEAR:
        zp = lax.rem(z + 8 - d, 8)
        if d:
            arrived(t_all.at[zp], r_a.at[zp])
        yd, side = zp // 2, lax.rem(zp, 2)
        xd = 2 * side + c
        rows = t_all[zp]
        for colour in range(2):
            part = dot(rows, wp[colour]).astype(B16)
            b1_out[zp, colour] = part
            if colour == 0:
                mine, dst, sem, to = xd == x, b1_in0.at[x, yd], r_b10.at[yd], (y, xd, z, c)
            else:
                mine, dst, sem, to = yd == y, b1_in1.at[y, side], r_b11.at[side], (yd, x, z, c)

            @pl.when(mine)
            def _():
                dst[...] = part

            put(b1_out.at[zp, colour], dst, sem, to, jnp.logical_not(mine))

    put(wu_h, wu.at[row_of, c], r_w.at[2], sibling)
    put(wd_h, wd.at[row_of, c], r_w.at[3], sibling)

    def first_stage_x(j):
        piece = lax.rem(z // 2 + j, 4)

        @pl.when(owner)
        def _():
            arrived(b1_in0.at[pl.ds(0, 3), piece], r_b10.at[piece])
            total = b1_in0[0, piece].astype(F32)
            for k in range(1, 4):
                total = total + b1_in0[k, piece].astype(F32)
            b2_out[j] = total.astype(B16)

        mine = jnp.logical_and(piece == y, c == 0)

        @pl.when(jnp.logical_and(owner, mine))
        def _():
            b2_in[y] = b2_out[j]

        put(
            b2_out.at[j], b2_in.at[y], r_b2.at[0], (piece, x, z, 0),
            jnp.logical_and(owner, jnp.logical_not(mine)),
        )

    def first_stage_y(j):
        side = lax.rem(z + j, 2)
        arrived(b1_in1.at[pl.ds(0, 3), side], r_b11.at[side])
        total = b1_in1[0, side].astype(F32)
        for k in range(1, 4):
            total = total + b1_in1[k, side].astype(F32)
        total = total.astype(B16)
        b2_out[4 + j] = total
        xd = 2 * side + c
        mine = jnp.logical_and(xd == x, c == 1)

        @pl.when(mine)
        def _():
            b2_in[x] = total

        put(b2_out.at[4 + j], b2_in.at[x], r_b2.at[0], (y, xd, z, 1), jnp.logical_not(mine))

    first_stage_x(0)
    first_stage_x(1)
    first_stage_y(0)
    first_stage_x(3)
    first_stage_y(1)
    first_stage_x(2)

    here[6].wait()
    to_partner(1)
    for i in (2, 3):
        arrived(theirs[i], r_w.at[i])
    gain_rows = jnp.broadcast_to(mixer_gain[...], (8, 256))
    for half in range(2):
        col_out[:, pl.ds(1024 * half, 1024)] = split_dot(gain_rows, wu[row_of, half], 3)[0:1]
    col_in[kv] = col_out[...]
    for k in (5, 7, 13, 15, 6, 14, 9, 11, 10, 1, 4, 3, 12, 2, 8):
        to = (lax.rem(y + k // 4, 4), lax.rem(x + k % 4, 4), z, c)
        put(col_out, col_in.at[kv], r_col.at[0], to)

    arrived(b2_in.at[pl.ds(0, 3)], r_b2.at[0], owner)
    arrived(b2_in, r_b2.at[0], jnp.logical_not(owner))
    qkvg = b2_in[0].astype(F32)
    for k in range(1, 4):
        qkvg = qkvg + b2_in[k].astype(F32)

    row_id = lax.broadcasted_iota(jnp.int32, (128, 128), 0)
    col_id = lax.broadcasted_iota(jnp.int32, (128, 128), 1)
    same_head = jnp.where(row_id // HDIM == col_id // HDIM, 1.0, 0.0).astype(B16)

    def rotated(u):
        partner = jnp.where(low, pltpu.roll(u, 96, 1), pltpu.roll(u, 32, 1))
        return u * cosine[...] + partner * sine[...]

    query, keyed, valued, gated = [
        qkvg[:, 128 * i : 128 * (i + 1)].astype(B16).astype(F32) for i in range(4)
    ]
    q_rot = rotated(query).astype(B16).astype(F32)
    k_rot = (rotated(keyed) * 0.125).astype(B16).astype(F32)
    own = split_dot(q_rot * k_rot, same_head, 2).astype(B16).astype(F32)
    turned[...] = q_rot
    retained[...] = own * valued
    for copy in here[7:]:
        copy.wait()
    pick_lane = lax.broadcasted_iota(jnp.int32, (HDIM, 128), 1)
    pick_row = lax.broadcasted_iota(jnp.int32, (HDIM, 128), 0)
    pick = jnp.where(lax.rem(pick_lane, HDIM) == pick_row, 1.0, 0.0)

    def attend(i, carry):
        rows = pl.ds(pl.multiple_of(i * 8, 8), 8)
        q = turned[rows, :]
        products = (keys[rows] * q.astype(B16)[:, None, :]).reshape(8 * BLK, 128)
        scores = dot(products, same_head).reshape(8, BLK, 128)
        weights = (scores * factor[rows]).astype(B16).astype(F32)
        inner = jnp.sum(weights * values[rows].astype(F32), axis=1)
        spread = (q[:, None, :] * pick[None]).reshape(8 * HDIM, 128).astype(B16)
        wide = dot(spread, same_head).reshape(8, HDIM, 128)
        cross = jnp.sum(wide * state[rows], axis=1)
        carried = jnp.exp(-rate * (offset[rows, :] + 1.0))
        retained[rows, :] += inner + cross * carried
        return carry

    lax.fori_loop(0, 8, attend, 0)
    kept = retained[...]
    centred = kept - split_dot(kept, same_head, 3) * (1.0 / HDIM)
    variance = split_dot(centred * centred, same_head, 3) * (1.0 / HDIM)
    normed = centred * lax.rsqrt(variance + EPS) * head_gain[...]
    mixed = (gated / (1.0 + jnp.exp(-gated)) * normed).astype(B16)
    heads[...] = mixed
    half = kv // 2

    for k in (10, 5, 7, 13, 15, 6, 14, 9, 11, 1, 4, 3, 12, 2, 8, 0):
        to = (lax.rem(y + k // 4, 4), lax.rem(x + k % 4, 4), z, row_of)
        put(heads, m_all.at[half, c], r_c.at[half], to, None if k else jnp.logical_not(owner))

    @pl.when(owner)
    def _():
        m_all[half, c] = mixed

    for k in range(2, 4):
        to_partner(k)
    on_to_sibling(0)

    here[4].wait()
    arrived(theirs[1], r_w.at[1])

    start = 2 * y + x // 2
    for j in (0, 1, 7, 2, 6, 3, 5, 4):
        i = lax.rem(start + j, 8)
        whole = 2 * i + c != kv
        arrived(m_all.at[i], r_c.at[i], whole)
        arrived(m_all.at[i, 0], r_c.at[i], jnp.logical_not(whole))
        part = (dot(m_all[i, 0], wo[0]) + dot(m_all[i, 1], wo[1])).astype(B16)
        mine = i == z

        @pl.when(mine)
        def _():
            d_in[i] = part

        d_out[i] = part
        put(d_out.at[i], d_in.at[z], r_d.at[0], (y, x, i, c), jnp.logical_not(mine))
    on_to_sibling(1)
    arrived(d_in.at[pl.ds(0, 7)], r_d.at[0])
    branch = d_in[z].astype(F32)
    for d in NEAR[1:]:
        i = lax.rem(z + 8 - d, 8)
        branch = branch + d_in[i].astype(F32)

    tall = ALPHA * tok[...].astype(F32) + branch
    part_mean = jnp.sum(tall, axis=1, keepdims=True) * (1.0 / 256)
    part_centred = tall - part_mean
    scaled = (part_centred * mixer_gain[...]).astype(B16)
    payload[...] = scaled
    turn = lax.rem(z, 2)
    stays = turn == row_of

    @pl.when(stays)
    def _():
        h_all[z // 2, row_of] = scaled

    for d in (4, 3, 5, 2, 6, 1, 7, 0):
        put(
            payload, h_all.at[z // 2, row_of], r_f.at[z // 2],
            (y, 2 * pair + turn, lax.rem(z + d, 8), c), None if d else jnp.logical_not(stays),
        )
    s_out[...] = packed_sums(part_mean, part_centred)[0:1]
    s_in[kv] = s_out[...]
    for k in (10, 5, 7, 13, 15, 6, 14, 9, 11, 1, 4, 3, 12, 2, 8):
        to = (lax.rem(y + k // 4, 4), lax.rem(x + k % 4, 4), z, c)
        put(s_out, s_in.at[kv], r_e.at[0], to)

    for k in range(2):
        arrived(chunk(k, 1 - row_of, 1 - c), r_v.at[k])

    along = (pair, y)
    size = (2, 4)

    def device_on(colour, stage, index):
        if (colour + stage) % 2 == 0:
            return (y, 2 * index + row_of, z, c)
        return (index, x, z, c)

    for d in range(4):
        t = lax.rem(z // 2 + (0, 1, 3, 2)[d], 4)
        whole = 2 * t + row_of != z
        arrived(h_all.at[t], r_f.at[t], whole)
        arrived(h_all.at[t, 0], r_f.at[t], jnp.logical_not(whole))
        for colour in range(2):
            part = (dot(h_all[t, 0], wu[0, colour]) + dot(h_all[t, 1], wu[1, colour])).astype(B16)
            for side in range(2):
                g1_out[colour, t, side] = part[32 * side : 32 * side + 32]
                spot = g1_out.at[colour, t, side]
                if colour == 0:
                    put(
                        spot, g1_inx.at[pair, t], r_g1x.at[t], device_on(0, 0, side),
                        pair != side,
                    )
                else:
                    put(spot, g1_iny.at[y, side], r_g1y.at[side], device_on(1, 0, t), y != t)

    arrived(s_in.at[pl.ds(0, 15)], r_e.at[0])
    shift, own_shift, scale = combined(s_out, s_in)
    eight = lax.broadcasted_iota(jnp.int32, (8, 128), 0)
    for group in range(2):
        stacked = jnp.zeros((8, 128), F32)
        for k in range(8):
            stacked = jnp.where(eight == k, shift[8 * group + k], stacked)
        p_out[group] = stacked
    p_out[2] = scale
    ends_at = 2 * y + row_of
    mine = ends_at == z

    @pl.when(mine)
    def _():
        p_in[...] = p_out[...]

    for d in range(1, 8):
        put(p_out, p_in, r_p.at[0], (y, x, lax.rem(z + d, 8), c), mine)
    wide_shift, wide_scale = column(own_shift)[:64], column(scale)[:64]
    hidden[...] = ((part_centred + wide_shift) * wide_scale * mixer_gain[...]).astype(B16)

    def first_sum(colour, j):
        me, other = along[colour], along[1 - colour]
        piece = lax.rem(other + j, size[1 - colour])
        total = (g1_out[0, piece, me] if colour == 0 else g1_out[1, me, piece]).astype(F32)
        if colour == 0:
            arrived(g1_inx.at[1 - pair, piece], r_g1x.at[piece])
            total = total + g1_inx[1 - pair, piece].astype(F32)
        else:
            arrived(g1_iny.at[pl.ds(0, 3), piece], r_g1y.at[piece])
            for d in (1, 3, 2):
                total = total + g1_iny[lax.rem(y + d, 4), piece].astype(F32)
        if j:
            g2_out[colour, piece] = total.astype(B16)
            put(
                g2_out.at[colour, piece], g2_in.at[colour, other], r_g2.at[colour],
                device_on(colour, 1, piece),
            )
        else:
            g_sum[colour] = total + lift[:, 1024 * colour : 1024 * colour + 1024]

    for colour, j in ((0, 2), (1, 1), (0, 1), (0, 3)):
        first_sum(colour, j)

    arrived(col_in.at[pl.ds(0, 15)], r_col.at[0])
    wide_eight = lax.broadcasted_iota(jnp.int32, (8, 2048), 0)
    arrived(p_in, r_p.at[0], jnp.logical_not(mine))
    lifted = jnp.zeros((128, 2048), F32)
    for group in range(2):
        stacked = jnp.zeros((8, 2048), F32)
        for k in range(8):
            stacked = jnp.where(wide_eight == k, col_in[8 * group + k], stacked)
        shift_high = p_in[group].astype(B16)
        shift_low = (p_in[group] - shift_high.astype(F32)).astype(B16)
        col_high = stacked.astype(B16)
        col_low = (stacked - col_high.astype(F32)).astype(B16)
        for a, b in ((shift_high, col_high), (shift_high, col_low), (shift_low, col_high)):
            lifted = lifted + lax.dot_general(a, b, (((0,), (0,)), ((), ())), preferred_element_type=F32)
    upper = pair == 1
    lift[...] = jnp.where(upper, lifted[32:64], lifted[:32])
    scales = column(p_in[2])
    ends[...] = jnp.where(upper, scales[32:64], scales[:32])

    for colour, j in ((0, 0), (1, 0)):
        first_sum(colour, j)
    for k in range(2, 4):
        on_to_sibling(k)

    def others(n):
        return (2, 1, 3) if n == 4 else (1,)

    for colour in range(2):
        me, other = along[colour], along[1 - colour]
        total = g_sum[colour]
        arrived(g2_in.at[colour, pl.ds(0, size[1 - colour] - 1)], r_g2.at[colour])
        for d in others(size[1 - colour]):
            source = lax.rem(other + d, size[1 - colour])
            total = total + g2_in[colour, source].astype(F32)
        times = jnp.concatenate([ends[...]] * 4, 1)
        active = jnp.square(jnp.maximum(total * times, 0.0)).astype(B16)
        spot = act_all.at[colour, y, pair]
        act_all[colour, y, pair] = active
        for stage in (1, 0):
            at = along[colour] if stage == 0 else along[1 - colour]
            n = size[(colour + stage) % 2]
            sem = r_h2.at[colour, y] if stage == 0 else r_h1.at[colour, other]
            for d in others(n):
                put(spot, spot, sem, device_on(colour, stage, lax.rem(at + d, n)))

    def forward(colour, j):
        me, other = along[colour], along[1 - colour]
        source = lax.rem(other + j, size[1 - colour])
        where = (source, pair) if colour == 0 else (y, source)
        spot = act_all.at[colour, where[0], where[1]]
        arrived(spot, r_h1.at[colour, source])
        for d in others(size[colour]):
            put(
                spot, spot, r_h2.at[colour, where[0]],
                device_on(colour, 0, lax.rem(me + d, size[colour])),
            )

    for colour, j in ((1, 1), (0, 1), (0, 3), (0, 2)):
        forward(colour, j)

    for k in range(2, 4):
        arrived(chunk(k, 1 - row_of, 1 - c), r_v.at[k])

    for j in range(4):
        t = y if j == 0 else j - 1 + (j - 1 >= y).astype(jnp.int32)
        arrived(act_all.at[0, t, 0], r_h2.at[0, t])
        if j:
            arrived(act_all.at[1, t], r_h2.at[1, t])
        upper_rows = act_all[0, t].reshape(64, 1024)
        lower_rows = act_all[1, t].reshape(64, 1024)
        for side in range(2):
            part = (dot(upper_rows, wd[side, 0]) + dot(lower_rows, wd[side, 1])).astype(B16)
            keep = jnp.logical_and(2 * t + row_of == z, row_of == side)
            e_out[t, side] = part

            @pl.when(keep)
            def _():
                e_in[z] = part

            put(
                e_out.at[t, side], e_in.at[z], r_i.at[0], (y, 2 * pair + side, 2 * t + row_of, c),
                jnp.logical_not(keep),
            )
    arrived(e_in.at[pl.ds(0, 7)], r_i.at[0], stays)
    arrived(e_in, r_i.at[0], jnp.logical_not(stays))
    downward = None
    for d in NEAR:
        i = lax.rem(z + 8 - d, 8)
        term = e_in[i].astype(F32)
        downward = term if downward is None else downward + term

    tall = ALPHA * hidden[...].astype(F32) + downward
    part_mean = jnp.sum(tall, axis=1, keepdims=True) * (1.0 / 256)
    part_centred = tall - part_mean
    j_out[...] = packed_sums(part_mean, part_centred)[0:1]
    j_in[kv] = j_out[...]
    for k in (10, 5, 7, 13, 15, 6, 14, 9, 11, 1, 4, 3, 12, 2, 8):
        to = (lax.rem(y + k // 4, 4), lax.rem(x + k % 4, 4), z, c)
        put(j_out, j_in.at[kv], r_j.at[0], to)
    arrived(j_in.at[pl.ds(0, 15)], r_j.at[0])
    shift, own_shift, scale = combined(j_out, j_in)
    wide_shift, wide_scale = column(own_shift)[:64], column(scale)[:64]
    out[...] = ((part_centred + wide_shift) * wide_scale * final_gain[...]).astype(B16)
    settle()


def per_device(
    tokens, lengths, state_block, cached_keys, cached_values, query_weight, key_weight,
    value_weight, gate_weight, decay_rate, head_gain, out_weight, mixer_gain, up_weight,
    down_weight, final_gain,
):
    vmem = pl.BlockSpec(memory_space=pltpu.VMEM)
    smem = pl.BlockSpec(memory_space=pltpu.SMEM)
    anywhere = pl.BlockSpec(memory_space=pl.ANY)
    dma = pltpu.SemaphoreType.DMA
    scratch = [
        pltpu.VMEM((64, 256), B16),
        pltpu.VMEM((1, 64), jnp.int32),
        pltpu.VMEM((1, 128), F32),
        pltpu.VMEM((1, 256), F32),
        pltpu.VMEM((1, 256), F32),
        pltpu.VMEM((64, 64, 128), F32),
        pltpu.VMEM((64, 128, 128), B16),
        pltpu.VMEM((64, 128, 128), B16),
        pltpu.VMEM((64, 128, 128), F32),
        pltpu.VMEM((2, 256, 512), B16),
        pltpu.VMEM((2, 128, 256), B16),
        pltpu.VMEM((2, 2, 256, 1024), B16),
        pltpu.VMEM((2, 2, 1024, 256), B16),
        pltpu.VMEM((64, 128), F32),
        pltpu.VMEM((64, 128), F32),
        pltpu.VMEM((64, 128), F32),
        pltpu.VMEM((8, 64, 256), B16),
        pltpu.VMEM((8, 2, 64, 512), B16),
        pltpu.VMEM((4, 4, 64, 512), B16),
        pltpu.VMEM((4, 2, 64, 512), B16),
        pltpu.VMEM((6, 64, 512), B16),
        pltpu.VMEM((4, 64, 512), B16),
        pltpu.VMEM((64, 128), F32),
        pltpu.VMEM((64, 128), F32),
        pltpu.VMEM((64, 128), B16),
        pltpu.VMEM((8, 2, 64, 128), B16),
        pltpu.VMEM((8, 64, 256), B16),
        pltpu.VMEM((8, 64, 256), B16),
        pltpu.VMEM((1, 128), F32),
        pltpu.VMEM((16, 1, 128), F32),
        pltpu.VMEM((3, 8, 128), F32),
        pltpu.VMEM((3, 8, 128), F32),
        pltpu.VMEM((1, 2048), F32),
        pltpu.VMEM((16, 1, 2048), F32),
        pltpu.VMEM((32, 256), F32),
        pltpu.VMEM((32, 2048), F32),
        pltpu.VMEM((64, 256), B16),
        pltpu.VMEM((64, 256), B16),
        pltpu.VMEM((4, 2, 64, 256), B16),
        pltpu.VMEM((2, 4, 2, 32, 1024), B16),
        pltpu.VMEM((2, 4, 32, 1024), B16),
        pltpu.VMEM((4, 2, 32, 1024), B16),
        pltpu.VMEM((2, 4, 32, 1024), B16),
        pltpu.VMEM((2, 4, 32, 1024), B16),
        pltpu.VMEM((2, 32, 1024), F32),
        pltpu.VMEM((2, 4, 2, 32, 1024), B16),
        pltpu.VMEM((4, 2, 64, 256), B16),
        pltpu.VMEM((8, 64, 256), B16),
        pltpu.VMEM((1, 128), F32),
        pltpu.VMEM((16, 1, 128), F32),
        dma((15,)),
        dma((SENDS,)),
        dma((4,)),
        dma((8,)),
        dma((4,)),
        dma((2,)),
        dma((1,)),
        dma((8,)),
        dma((1,)),
        dma((1,)),
        dma((1,)),
        dma((1,)),
        dma((4,)),
        dma((4,)),
        dma((2,)),
        dma((2,)),
        dma((2, 4)),
        dma((2, 4)),
        dma((1,)),
        dma((1,)),
        dma((4,)),
        dma((4,)),
    ]
    return pl.pallas_call(
        kernel,
        out_shape=jax.ShapeDtypeStruct((64, 256), B16),
        in_specs=[anywhere] * 5 + [smem] + [anywhere] * 10,
        out_specs=vmem,
        scratch_shapes=scratch,
        name="layer",
        compiler_params=pltpu.CompilerParams(
            collective_id=0, has_side_effects=True, vmem_limit_bytes=56 * 1024 * 1024
        ),
    )(
        tokens, lengths[None, :], head_gain[None, :], mixer_gain[None, :], final_gain[None, :], decay_rate,
        state_block, cached_keys, cached_values, query_weight, key_weight, value_weight, gate_weight,
        out_weight, up_weight, down_weight,
    )


def solution(mesh):
    finer = Mesh(mesh.devices.reshape(4, 4, 8, 2), AXES)
    kv, tp = ("y", "x"), ("z", "c")
    placed = (
        P(tp, kv), P(kv), P(kv, None, tp), P(kv, None, tp), P(kv, None, tp),
        P(kv, tp), P(kv, tp), P(kv, tp), P(kv, tp), P(tp), P(tp), P(tp, kv), P(kv),
        P(kv, tp), P(tp, kv), P(kv),
    )
    return jax.shard_map(per_device, mesh=finer, in_specs=placed, out_specs=P(tp, kv), check_vma=False)
```

```python
import functools

import jax
import jax.numpy as jnp
from jax import lax
from jax.experimental import pallas as pl
from jax.experimental.pallas import tpu as pltpu
from jax.sharding import Mesh
from jax.sharding import PartitionSpec as P

HDIM = 64
BLK = 128
ALPHA = 2.0**0.5
EPS = 1e-05
AXES = ("y", "x", "z", "c")
NEAR = (0, 1, 7, 2, 6, 3, 5, 4)
POOL = 32
SENDS = 36
F32 = jnp.float32
B16 = jnp.bfloat16


def dot(a, b):
    return jnp.dot(a, b, preferred_element_type=F32)


def split_dot(a, b, terms, left=True):
    total = None
    rest = a if left else b
    for _ in range(terms):
        part = rest.astype(B16)
        rest = rest - part.astype(F32)
        term = dot(part, b) if left else dot(a, part)
        total = term if total is None else total + term
    return total


def copy_to(src, dst, send, recv, device):
    return pltpu.make_async_remote_copy(
        src_ref=src,
        dst_ref=dst,
        send_sem=send,
        recv_sem=recv,
        device_id=device,
        device_id_type=pl.DeviceIdType.MESH,
    )


def kernel(
    tok_h, lengths_h, head_gain_h, mixer_gain_h, final_gain_h, rates,
    state_h, keys_h, values_h, wq_h, wk_h, wv_h, wg_h, wo_h, wu_h, wd_h,
    out,
    tok, lengths, head_gain, mixer_gain, final_gain, state, keys, values, factor, wp, wo, wu, wd, cosine, sine, offset,
    t_all, b1_out, b1_in0, b1_in1, b2_out, b2_in, retained, turned, heads, m_all, d_out, d_in,
    s_out, s_in, p_out, p_in, col_out, col_in, ends, lift, payload, hidden, h_all,
    g1_out, g1_inx, g1_iny, g2_out, g2_in, g_sum, act_all, e_out, e_in, j_out, j_in,
    local, send, r_w, r_a, r_b10, r_b11, r_b2, r_c, r_d, r_e, r_p, r_col, r_f,
    r_g1x, r_g1y, r_g2, r_h1, r_h2, r_i, r_j, r_x, r_v,
):
    y, x, z, c = [lax.axis_index(name) for name in AXES]
    kv = y * 4 + x
    sibling = (y, x, z, 1 - c)
    row_of = lax.rem(x, 2)
    owner = row_of == c
    pair = x // 2
    partner = (y, 2 * pair + 1 - row_of, z, c)
    pending = [None] * SENDS
    used = [0]

    def sent(slot):
        if pending[slot] is None:
            return
        when, copy = pending[slot]
        pending[slot] = None
        if when is None:
            copy.wait_send()
        else:

            @pl.when(when)
            def _():
                copy.wait_send()

    def put(src, dst, recv, device, when=None, slot=None):
        if slot is None:
            slot = used[0] % POOL
            used[0] += 1
        sent(slot)
        copy = copy_to(src, dst, send.at[slot], recv, device)
        if when is None:
            copy.start()
        else:

            @pl.when(when)
            def _():
                copy.start()

        pending[slot] = (when, copy)

    def settle():
        for slot in range(SENDS):
            sent(slot)

    def arrived(dst, sem, when=None):
        copy = copy_to(dst, dst, send.at[0], sem, sibling)
        if when is None:
            copy.wait_recv()
        else:

            @pl.when(when)
            def _():
                copy.wait_recv()

    barrier = pltpu.get_barrier_semaphore()
    greeted = 0
    for dy in range(4):
        for dx in range(4):
            for dc in range(2):
                if dy or dx or dc:
                    peer = (lax.rem(y + dy, 4), lax.rem(x + dx, 4), z, lax.rem(c + dc, 2))
                    pl.semaphore_signal(barrier, inc=1, device_id=peer, device_id_type=pl.DeviceIdType.MESH)
                    greeted += 1
    for dz in range(1, 8):
        peer = (y, x, lax.rem(z + dz, 8), c)
        pl.semaphore_signal(barrier, inc=1, device_id=peer, device_id_type=pl.DeviceIdType.MESH)
        greeted += 1
        peer = (y, 2 * pair + 1 - row_of, lax.rem(z + dz, 8), c)
        pl.semaphore_signal(barrier, inc=1, device_id=peer, device_id_type=pl.DeviceIdType.MESH)
        greeted += 1

    small = []
    for src, dst in (
        (lengths_h, lengths), (tok_h, tok), (head_gain_h, head_gain), (mixer_gain_h, mixer_gain),
        (final_gain_h, final_gain),
    ):
        small.append(pltpu.make_async_copy(src, dst, local.at[10 + len(small)]))
        small[-1].start()

    here = []

    def fetch(src, dst):
        here.append(pltpu.make_async_copy(src, dst, local.at[len(here)]))
        here[-1].start()

    quarter = [wp.at[c, :, pl.ds(128 * i, 128)] for i in range(4)]
    for src, dst in zip((wq_h, wk_h, wv_h, wg_h), quarter):
        fetch(src, dst)
    fetch(wo_h, wo.at[c])
    fetch(wu_h, wu.at[row_of, c])
    fetch(wd_h, wd.at[row_of, c])
    fetch(keys_h, keys)
    fetch(values_h, values)
    fetch(state_h, state)

    ones = jnp.full((8, 256), 1.0, B16)
    first = jnp.where(lax.broadcasted_iota(jnp.int32, (8, 256), 0) == 0, 1.0, 0.0).astype(B16)
    lane = lax.broadcasted_iota(jnp.int32, (64, 128), 1)
    low = lax.rem(lane, HDIM) < HDIM // 2
    lane_row = lax.broadcasted_iota(jnp.int32, (1, 128), 1)
    rate = jnp.where(lane_row < HDIM, rates[0], rates[1])

    def row_sums(u):
        total = None
        for _ in range(3):
            part = u.astype(B16)
            u = u - part.astype(F32)
            term = lax.dot_general(ones, part, (((1,), (1,)), ((), ())), preferred_element_type=F32)
            total = term if total is None else total + term
        return total

    def packed_sums(part_mean, part_centred):
        means = jnp.broadcast_to(part_mean * (1.0 / 256), (64, 256))
        return row_sums(jnp.concatenate([means, part_centred * part_centred], 0))

    def combined(own_sums, sums):
        total = jnp.sum(sums[...], axis=0)
        mean = total * (1.0 / 16)
        shift = jnp.where((lane_row < 64)[None], sums[...] - mean[None], 0.0)
        between = jnp.sum(shift * shift, axis=0)
        spread = (pltpu.roll(total, 64, 1) + 256.0 * between) * (1.0 / 4096)
        scale = jnp.where(lane_row < 64, lax.rsqrt(spread + EPS), 0.0)
        own_shift = jnp.broadcast_to(jnp.where(lane_row < 64, own_sums[...] - mean, 0.0), (8, 128))
        return shift, own_shift, jnp.broadcast_to(scale, (8, 128))

    def column(u):
        total = None
        for _ in range(3):
            part = u.astype(B16)
            u = u - part.astype(F32)
            term = lax.dot_general(part, first, (((0,), (0,)), ((), ())), preferred_element_type=F32)
            total = term if total is None else total + term
        return total

    small[0].wait()
    position = column(jnp.broadcast_to(lengths[...].astype(F32), (8, 64)))[:, :128]
    offset[...] = position - jnp.floor(position * (1.0 / BLK)) * BLK
    inverse = jnp.zeros((1, 128), F32)
    for i in range(HDIM // 2):
        inverse = jnp.where(lax.rem(lane_row, HDIM // 2) == i, 10000.0 ** (-i / (HDIM // 2)), inverse)
    angle = position * inverse
    cosine[...] = jnp.cos(angle)
    sines = jnp.sin(angle)
    sine[...] = jnp.where(low, -sines, sines)

    def decay(i, carry):
        rows = pl.ds(pl.multiple_of(i * 8, 8), 8)
        off = offset[rows, :][:, None, :]
        slot = lax.broadcasted_iota(jnp.int32, (8, BLK, 128), 1).astype(F32)
        lag = jnp.maximum(off - slot, 0.0)
        factor[rows] = jnp.where(slot < off, jnp.exp(-rate[None] * lag), 0.0)
        return carry

    lax.fori_loop(0, 8, decay, 0)
    for copy in small[1:]:
        copy.wait()
    t_all[z] = tok[...]
    pl.semaphore_wait(barrier, greeted)

    for d in (1, 7, 2, 6):
        put(tok, t_all.at[z], r_a.at[z], (y, x, lax.rem(z + d, 8), c))
    for i, (src, dst) in enumerate(
        [*zip((wq_h, wk_h, wv_h, wg_h), quarter), (wo_h, wo.at[c])]
    ):
        put(src, dst, r_w.at[max(i - 3, 0)], sibling)
    theirs = [wp.at[1 - c], wo.at[1 - c], wu.at[row_of, 1 - c], wd.at[row_of, 1 - c]]
    def chunk(k, side, core):
        if k < 2:
            return wu.at[side, core, pl.ds(128 * k, 128), :]
        return wd.at[side, core, pl.ds(512 * (k - 2), 512), :]

    def to_partner(k):
        put(chunk(k, row_of, c), chunk(k, row_of, c), r_x.at[k], partner, slot=POOL + k)

    def on_to_sibling(k):
        arrived(chunk(k, 1 - row_of, c), r_x.at[k])
        put(chunk(k, 1 - row_of, c), chunk(k, 1 - row_of, c), r_v.at[k], sibling)

    here[5].wait()
    to_partner(0)
    for i in range(4):
        here[i].wait()
    arrived(theirs[0], r_w.at[0])

    for d in NEAR:
        zp = lax.rem(z + 8 - d, 8)
        if d:
            arrived(t_all.at[zp], r_a.at[zp])
        for further in {2: (1, 2), 6: (7,)}.get(d, ()):
            put(t_all.at[zp], t_all.at[zp], r_a.at[zp], (y, x, lax.rem(z + further, 8), c))
        yd, side = zp // 2, lax.rem(zp, 2)
        xd = 2 * side + c
        rows = t_all[zp]
        for colour in range(2):
            part = dot(rows, wp[colour]).astype(B16)
            b1_out[zp, colour] = part
            if colour == 0:
                mine, dst, sem, to = xd == x, b1_in0.at[x, yd], r_b10.at[yd], (y, xd, z, c)
            else:
                mine, dst, sem, to = yd == y, b1_in1.at[y, side], r_b11.at[side], (yd, x, z, c)

            @pl.when(mine)
            def _():
                dst[...] = part

            put(b1_out.at[zp, colour], dst, sem, to, jnp.logical_not(mine))

    put(wu_h, wu.at[row_of, c], r_w.at[2], sibling)
    put(wd_h, wd.at[row_of, c], r_w.at[3], sibling)

    def first_stage_x(j):
        piece = lax.rem(z // 2 + j, 4)

        @pl.when(owner)
        def _():
            arrived(b1_in0.at[pl.ds(0, 3), piece], r_b10.at[piece])
            total = b1_in0[0, piece].astype(F32)
            for k in range(1, 4):
                total = total + b1_in0[k, piece].astype(F32)
            b2_out[j] = total.astype(B16)

        mine = jnp.logical_and(piece == y, c == 0)

        @pl.when(jnp.logical_and(owner, mine))
        def _():
            b2_in[y] = b2_out[j]

        put(
            b2_out.at[j], b2_in.at[y], r_b2.at[0], (piece, x, z, 0),
            jnp.logical_and(owner, jnp.logical_not(mine)),
        )

    def first_stage_y(j):
        side = lax.rem(z + j, 2)
        arrived(b1_in1.at[pl.ds(0, 3), side], r_b11.at[side])
        total = b1_in1[0, side].astype(F32)
        for k in range(1, 4):
            total = total + b1_in1[k, side].astype(F32)
        total = total.astype(B16)
        b2_out[4 + j] = total
        xd = 2 * side + c
        mine = jnp.logical_and(xd == x, c == 1)

        @pl.when(mine)
        def _():
            b2_in[x] = total

        put(b2_out.at[4 + j], b2_in.at[x], r_b2.at[0], (y, xd, z, 1), jnp.logical_not(mine))

    first_stage_x(0)
    first_stage_x(1)
    first_stage_y(0)
    first_stage_x(3)
    first_stage_y(1)
    first_stage_x(2)

    here[6].wait()
    to_partner(1)
    for i in (2, 3):
        arrived(theirs[i], r_w.at[i])
    gain_rows = jnp.broadcast_to(mixer_gain[...], (8, 256))
    for half in range(2):
        col_out[:, pl.ds(1024 * half, 1024)] = split_dot(gain_rows, wu[row_of, half], 3)[0:1]
    col_in[kv] = col_out[...]
    for k in (5, 7, 13, 15, 6, 14, 9, 11, 10, 1, 4, 3, 12, 2, 8):
        to = (lax.rem(y + k // 4, 4), lax.rem(x + k % 4, 4), z, c)
        put(col_out, col_in.at[kv], r_col.at[0], to)

    arrived(b2_in.at[pl.ds(0, 3)], r_b2.at[0], owner)
    arrived(b2_in, r_b2.at[0], jnp.logical_not(owner))
    qkvg = b2_in[0].astype(F32)
    for k in range(1, 4):
        qkvg = qkvg + b2_in[k].astype(F32)

    row_id = lax.broadcasted_iota(jnp.int32, (128, 128), 0)
    col_id = lax.broadcasted_iota(jnp.int32, (128, 128), 1)
    same_head = jnp.where(row_id // HDIM == col_id // HDIM, 1.0, 0.0).astype(B16)

    def rotated(u):
        partner = jnp.where(low, pltpu.roll(u, 96, 1), pltpu.roll(u, 32, 1))
        return u * cosine[...] + partner * sine[...]

    query, keyed, valued, gated = [
        qkvg[:, 128 * i : 128 * (i + 1)].astype(B16).astype(F32) for i in range(4)
    ]
    q_rot = rotated(query).astype(B16).astype(F32)
    k_rot = (rotated(keyed) * 0.125).astype(B16).astype(F32)
    own = split_dot(q_rot * k_rot, same_head, 2).astype(B16).astype(F32)
    turned[...] = q_rot
    retained[...] = own * valued
    for copy in here[7:]:
        copy.wait()
    pick_lane = lax.broadcasted_iota(jnp.int32, (HDIM, 128), 1)
    pick_row = lax.broadcasted_iota(jnp.int32, (HDIM, 128), 0)
    pick = jnp.where(lax.rem(pick_lane, HDIM) == pick_row, 1.0, 0.0)

    def attend(i, carry):
        rows = pl.ds(pl.multiple_of(i * 8, 8), 8)
        q = turned[rows, :]
        products = (keys[rows] * q.astype(B16)[:, None, :]).reshape(8 * BLK, 128)
        scores = dot(products, same_head).reshape(8, BLK, 128)
        weights = (scores * factor[rows]).astype(B16).astype(F32)
        inner = jnp.sum(weights * values[rows].astype(F32), axis=1)
        spread = (q[:, None, :] * pick[None]).reshape(8 * HDIM, 128).astype(B16)
        wide = dot(spread, same_head).reshape(8, HDIM, 128)
        cross = jnp.sum(wide * state[rows], axis=1)
        carried = jnp.exp(-rate * (offset[rows, :] + 1.0))
        retained[rows, :] += inner + cross * carried
        return carry

    lax.fori_loop(0, 8, attend, 0)
    kept = retained[...]
    centred = kept - split_dot(kept, same_head, 3) * (1.0 / HDIM)
    variance = split_dot(centred * centred, same_head, 3) * (1.0 / HDIM)
    normed = centred * lax.rsqrt(variance + EPS) * head_gain[...]
    mixed = (gated / (1.0 + jnp.exp(-gated)) * normed).astype(B16)
    heads[...] = mixed
    half = kv // 2

    for k in (10, 5, 7, 13, 15, 6, 14, 9, 11, 1, 4, 3, 12, 2, 8, 0):
        to = (lax.rem(y + k // 4, 4), lax.rem(x + k % 4, 4), z, row_of)
        put(heads, m_all.at[half, c], r_c.at[half], to, None if k else jnp.logical_not(owner))

    @pl.when(owner)
    def _():
        m_all[half, c] = mixed

    for k in range(2, 4):
        to_partner(k)
    on_to_sibling(0)

    here[4].wait()
    arrived(theirs[1], r_w.at[1])

    start = 2 * y + x // 2
    for j in (0, 1, 7, 2, 6, 3, 5, 4):
        i = lax.rem(start + j, 8)
        whole = 2 * i + c != kv
        arrived(m_all.at[i], r_c.at[i], whole)
        arrived(m_all.at[i, 0], r_c.at[i], jnp.logical_not(whole))
        part = (dot(m_all[i, 0], wo[0]) + dot(m_all[i, 1], wo[1])).astype(B16)
        mine = i == z

        @pl.when(mine)
        def _():
            d_in[i] = part

        d_out[i] = part
        put(d_out.at[i], d_in.at[z], r_d.at[0], (y, x, i, c), jnp.logical_not(mine))
    on_to_sibling(1)
    arrived(d_in.at[pl.ds(0, 7)], r_d.at[0])
    branch = d_in[z].astype(F32)
    for d in NEAR[1:]:
        i = lax.rem(z + 8 - d, 8)
        branch = branch + d_in[i].astype(F32)

    tall = ALPHA * tok[...].astype(F32) + branch
    part_mean = jnp.sum(tall, axis=1, keepdims=True) * (1.0 / 256)
    part_centred = tall - part_mean
    scaled = (part_centred * mixer_gain[...]).astype(B16)
    payload[...] = scaled
    turn = lax.rem(z, 2)
    stays = turn == row_of

    @pl.when(stays)
    def _():
        h_all[z // 2, row_of] = scaled

    for d in (4, 3, 5, 2, 6, 1, 7, 0):
        put(
            payload, h_all.at[z // 2, row_of], r_f.at[z // 2],
            (y, 2 * pair + turn, lax.rem(z + d, 8), c), None if d else jnp.logical_not(stays),
        )
    s_out[...] = packed_sums(part_mean, part_centred)[0:1]
    s_in[kv] = s_out[...]
    for k in (10, 5, 7, 13, 15, 6, 14, 9, 11, 1, 4, 3, 12, 2, 8):
        to = (lax.rem(y + k // 4, 4), lax.rem(x + k % 4, 4), z, c)
        put(s_out, s_in.at[kv], r_e.at[0], to)

    for k in range(2):
        arrived(chunk(k, 1 - row_of, 1 - c), r_v.at[k])

    along = (pair, y)
    size = (2, 4)

    def device_on(colour, stage, index):
        if (colour + stage) % 2 == 0:
            return (y, 2 * index + row_of, z, c)
        return (index, x, z, c)

    for d in range(4):
        t = lax.rem(z // 2 + (0, 1, 3, 2)[d], 4)
        whole = 2 * t + row_of != z
        arrived(h_all.at[t], r_f.at[t], whole)
        arrived(h_all.at[t, 0], r_f.at[t], jnp.logical_not(whole))
        for colour in range(2):
            part = (dot(h_all[t, 0], wu[0, colour]) + dot(h_all[t, 1], wu[1, colour])).astype(B16)
            for side in range(2):
                g1_out[colour, t, side] = part[32 * side : 32 * side + 32]
                spot = g1_out.at[colour, t, side]
                if colour == 0:
                    put(
                        spot, g1_inx.at[pair, t], r_g1x.at[t], device_on(0, 0, side),
                        pair != side,
                    )
                else:
                    put(spot, g1_iny.at[y, side], r_g1y.at[side], device_on(1, 0, t), y != t)

    arrived(s_in.at[pl.ds(0, 15)], r_e.at[0])
    shift, own_shift, scale = combined(s_out, s_in)
    eight = lax.broadcasted_iota(jnp.int32, (8, 128), 0)
    for group in range(2):
        stacked = jnp.zeros((8, 128), F32)
        for k in range(8):
            stacked = jnp.where(eight == k, shift[8 * group + k], stacked)
        p_out[group] = stacked
    p_out[2] = scale
    ends_at = 2 * y + row_of
    mine = ends_at == z

    @pl.when(mine)
    def _():
        p_in[...] = p_out[...]

    for d in range(1, 8):
        put(p_out, p_in, r_p.at[0], (y, x, lax.rem(z + d, 8), c), mine)
    wide_shift, wide_scale = column(own_shift)[:64], column(scale)[:64]
    hidden[...] = ((part_centred + wide_shift) * wide_scale * mixer_gain[...]).astype(B16)

    def first_sum(colour, j):
        me, other = along[colour], along[1 - colour]
        piece = lax.rem(other + j, size[1 - colour])
        total = (g1_out[0, piece, me] if colour == 0 else g1_out[1, me, piece]).astype(F32)
        if colour == 0:
            arrived(g1_inx.at[1 - pair, piece], r_g1x.at[piece])
            total = total + g1_inx[1 - pair, piece].astype(F32)
        else:
            arrived(g1_iny.at[pl.ds(0, 3), piece], r_g1y.at[piece])
            for d in (1, 3, 2):
                total = total + g1_iny[lax.rem(y + d, 4), piece].astype(F32)
        if j:
            g2_out[colour, piece] = total.astype(B16)
            put(
                g2_out.at[colour, piece], g2_in.at[colour, other], r_g2.at[colour],
                device_on(colour, 1, piece),
            )
        else:
            g_sum[colour] = total + lift[:, 1024 * colour : 1024 * colour + 1024]

    for colour, j in ((0, 2), (1, 1), (0, 1), (0, 3)):
        first_sum(colour, j)

    arrived(col_in.at[pl.ds(0, 15)], r_col.at[0])
    wide_eight = lax.broadcasted_iota(jnp.int32, (8, 2048), 0)
    arrived(p_in, r_p.at[0], jnp.logical_not(mine))
    lifted = jnp.zeros((128, 2048), F32)
    for group in range(2):
        stacked = jnp.zeros((8, 2048), F32)
        for k in range(8):
            stacked = jnp.where(wide_eight == k, col_in[8 * group + k], stacked)
        shift_high = p_in[group].astype(B16)
        shift_low = (p_in[group] - shift_high.astype(F32)).astype(B16)
        col_high = stacked.astype(B16)
        col_low = (stacked - col_high.astype(F32)).astype(B16)
        for a, b in ((shift_high, col_high), (shift_high, col_low), (shift_low, col_high)):
            lifted = lifted + lax.dot_general(a, b, (((0,), (0,)), ((), ())), preferred_element_type=F32)
    upper = pair == 1
    lift[...] = jnp.where(upper, lifted[32:64], lifted[:32])
    scales = column(p_in[2])
    ends[...] = jnp.where(upper, scales[32:64], scales[:32])

    for colour, j in ((0, 0), (1, 0)):
        first_sum(colour, j)
    for k in range(2, 4):
        on_to_sibling(k)

    def others(n):
        return (2, 1, 3) if n == 4 else (1,)

    for colour in range(2):
        me, other = along[colour], along[1 - colour]
        total = g_sum[colour]
        arrived(g2_in.at[colour, pl.ds(0, size[1 - colour] - 1)], r_g2.at[colour])
        for d in others(size[1 - colour]):
            source = lax.rem(other + d, size[1 - colour])
            total = total + g2_in[colour, source].astype(F32)
        times = jnp.concatenate([ends[...]] * 4, 1)
        active = jnp.square(jnp.maximum(total * times, 0.0)).astype(B16)
        spot = act_all.at[colour, y, pair]
        act_all[colour, y, pair] = active
        for stage in (1, 0):
            at = along[colour] if stage == 0 else along[1 - colour]
            n = size[(colour + stage) % 2]
            sem = r_h2.at[colour, y] if stage == 0 else r_h1.at[colour, other]
            for d in others(n):
                put(spot, spot, sem, device_on(colour, stage, lax.rem(at + d, n)))

    def forward(colour, j):
        me, other = along[colour], along[1 - colour]
        source = lax.rem(other + j, size[1 - colour])
        where = (source, pair) if colour == 0 else (y, source)
        spot = act_all.at[colour, where[0], where[1]]
        arrived(spot, r_h1.at[colour, source])
        for d in others(size[colour]):
            put(
                spot, spot, r_h2.at[colour, where[0]],
                device_on(colour, 0, lax.rem(me + d, size[colour])),
            )

    for colour, j in ((1, 1), (0, 1), (0, 3), (0, 2)):
        forward(colour, j)

    for k in range(2, 4):
        arrived(chunk(k, 1 - row_of, 1 - c), r_v.at[k])

    for j in range(4):
        t = y if j == 0 else j - 1 + (j - 1 >= y).astype(jnp.int32)
        arrived(act_all.at[0, t, 0], r_h2.at[0, t])
        if j:
            arrived(act_all.at[1, t], r_h2.at[1, t])
        upper_rows = act_all[0, t].reshape(64, 1024)
        lower_rows = act_all[1, t].reshape(64, 1024)
        for side in range(2):
            part = (dot(upper_rows, wd[side, 0]) + dot(lower_rows, wd[side, 1])).astype(B16)
            keep = jnp.logical_and(2 * t + row_of == z, row_of == side)
            e_out[t, side] = part

            @pl.when(keep)
            def _():
                e_in[z] = part

            put(
                e_out.at[t, side], e_in.at[z], r_i.at[0], (y, 2 * pair + side, 2 * t + row_of, c),
                jnp.logical_not(keep),
            )
    arrived(e_in.at[pl.ds(0, 7)], r_i.at[0], stays)
    arrived(e_in, r_i.at[0], jnp.logical_not(stays))
    downward = None
    for d in NEAR:
        i = lax.rem(z + 8 - d, 8)
        term = e_in[i].astype(F32)
        downward = term if downward is None else downward + term

    tall = ALPHA * hidden[...].astype(F32) + downward
    part_mean = jnp.sum(tall, axis=1, keepdims=True) * (1.0 / 256)
    part_centred = tall - part_mean
    j_out[...] = packed_sums(part_mean, part_centred)[0:1]
    j_in[kv] = j_out[...]
    for k in (10, 5, 7, 13, 15, 6, 14, 9, 11, 1, 4, 3, 12, 2, 8):
        to = (lax.rem(y + k // 4, 4), lax.rem(x + k % 4, 4), z, c)
        put(j_out, j_in.at[kv], r_j.at[0], to)
    arrived(j_in.at[pl.ds(0, 15)], r_j.at[0])
    shift, own_shift, scale = combined(j_out, j_in)
    wide_shift, wide_scale = column(own_shift)[:64], column(scale)[:64]
    out[...] = ((part_centred + wide_shift) * wide_scale * final_gain[...]).astype(B16)
    settle()


def per_device(
    tokens, lengths, state_block, cached_keys, cached_values, query_weight, key_weight,
    value_weight, gate_weight, decay_rate, head_gain, out_weight, mixer_gain, up_weight,
    down_weight, final_gain,
):
    vmem = pl.BlockSpec(memory_space=pltpu.VMEM)
    smem = pl.BlockSpec(memory_space=pltpu.SMEM)
    anywhere = pl.BlockSpec(memory_space=pl.ANY)
    dma = pltpu.SemaphoreType.DMA
    scratch = [
        pltpu.VMEM((64, 256), B16),
        pltpu.VMEM((1, 64), jnp.int32),
        pltpu.VMEM((1, 128), F32),
        pltpu.VMEM((1, 256), F32),
        pltpu.VMEM((1, 256), F32),
        pltpu.VMEM((64, 64, 128), F32),
        pltpu.VMEM((64, 128, 128), B16),
        pltpu.VMEM((64, 128, 128), B16),
        pltpu.VMEM((64, 128, 128), F32),
        pltpu.VMEM((2, 256, 512), B16),
        pltpu.VMEM((2, 128, 256), B16),
        pltpu.VMEM((2, 2, 256, 1024), B16),
        pltpu.VMEM((2, 2, 1024, 256), B16),
        pltpu.VMEM((64, 128), F32),
        pltpu.VMEM((64, 128), F32),
        pltpu.VMEM((64, 128), F32),
        pltpu.VMEM((8, 64, 256), B16),
        pltpu.VMEM((8, 2, 64, 512), B16),
        pltpu.VMEM((4, 4, 64, 512), B16),
        pltpu.VMEM((4, 2, 64, 512), B16),
        pltpu.VMEM((6, 64, 512), B16),
        pltpu.VMEM((4, 64, 512), B16),
        pltpu.VMEM((64, 128), F32),
        pltpu.VMEM((64, 128), F32),
        pltpu.VMEM((64, 128), B16),
        pltpu.VMEM((8, 2, 64, 128), B16),
        pltpu.VMEM((8, 64, 256), B16),
        pltpu.VMEM((8, 64, 256), B16),
        pltpu.VMEM((1, 128), F32),
        pltpu.VMEM((16, 1, 128), F32),
        pltpu.VMEM((3, 8, 128), F32),
        pltpu.VMEM((3, 8, 128), F32),
        pltpu.VMEM((1, 2048), F32),
        pltpu.VMEM((16, 1, 2048), F32),
        pltpu.VMEM((32, 256), F32),
        pltpu.VMEM((32, 2048), F32),
        pltpu.VMEM((64, 256), B16),
        pltpu.VMEM((64, 256), B16),
        pltpu.VMEM((4, 2, 64, 256), B16),
        pltpu.VMEM((2, 4, 2, 32, 1024), B16),
        pltpu.VMEM((2, 4, 32, 1024), B16),
        pltpu.VMEM((4, 2, 32, 1024), B16),
        pltpu.VMEM((2, 4, 32, 1024), B16),
        pltpu.VMEM((2, 4, 32, 1024), B16),
        pltpu.VMEM((2, 32, 1024), F32),
        pltpu.VMEM((2, 4, 2, 32, 1024), B16),
        pltpu.VMEM((4, 2, 64, 256), B16),
        pltpu.VMEM((8, 64, 256), B16),
        pltpu.VMEM((1, 128), F32),
        pltpu.VMEM((16, 1, 128), F32),
        dma((15,)),
        dma((SENDS,)),
        dma((4,)),
        dma((8,)),
        dma((4,)),
        dma((2,)),
        dma((1,)),
        dma((8,)),
        dma((1,)),
        dma((1,)),
        dma((1,)),
        dma((1,)),
        dma((4,)),
        dma((4,)),
        dma((2,)),
        dma((2,)),
        dma((2, 4)),
        dma((2, 4)),
        dma((1,)),
        dma((1,)),
        dma((4,)),
        dma((4,)),
    ]
    return pl.pallas_call(
        kernel,
        out_shape=jax.ShapeDtypeStruct((64, 256), B16),
        in_specs=[anywhere] * 5 + [smem] + [anywhere] * 10,
        out_specs=vmem,
        scratch_shapes=scratch,
        name="layer",
        compiler_params=pltpu.CompilerParams(
            collective_id=0, has_side_effects=True, vmem_limit_bytes=56 * 1024 * 1024
        ),
    )(
        tokens, lengths[None, :], head_gain[None, :], mixer_gain[None, :], final_gain[None, :], decay_rate,
        state_block, cached_keys, cached_values, query_weight, key_weight, value_weight, gate_weight,
        out_weight, up_weight, down_weight,
    )


def solution(mesh):
    finer = Mesh(mesh.devices.reshape(4, 4, 8, 2), AXES)
    kv, tp = ("y", "x"), ("z", "c")
    placed = (
        P(tp, kv), P(kv), P(kv, None, tp), P(kv, None, tp), P(kv, None, tp),
        P(kv, tp), P(kv, tp), P(kv, tp), P(kv, tp), P(tp), P(tp), P(tp, kv), P(kv),
        P(kv, tp), P(tp, kv), P(kv),
    )
    return jax.shard_map(per_device, mesh=finer, in_specs=placed, out_specs=P(tp, kv), check_vma=False)
```

```python
import functools

import jax
import jax.numpy as jnp
from jax import lax
from jax.experimental import pallas as pl
from jax.experimental.pallas import tpu as pltpu
from jax.sharding import Mesh
from jax.sharding import PartitionSpec as P

HDIM = 64
BLK = 128
ALPHA = 2.0**0.5
EPS = 1e-05
AXES = ("y", "x", "z", "c")
NEAR = (0, 1, 7, 2, 6, 3, 5, 4)
POOL = 32
SENDS = 36
F32 = jnp.float32
B16 = jnp.bfloat16


def dot(a, b):
    return jnp.dot(a, b, preferred_element_type=F32)


def split_dot(a, b, terms, left=True):
    total = None
    rest = a if left else b
    for _ in range(terms):
        part = rest.astype(B16)
        rest = rest - part.astype(F32)
        term = dot(part, b) if left else dot(a, part)
        total = term if total is None else total + term
    return total


def copy_to(src, dst, send, recv, device):
    return pltpu.make_async_remote_copy(
        src_ref=src,
        dst_ref=dst,
        send_sem=send,
        recv_sem=recv,
        device_id=device,
        device_id_type=pl.DeviceIdType.MESH,
    )


def kernel(
    tok_h, lengths_h, head_gain_h, mixer_gain_h, final_gain_h, rates,
    state_h, keys_h, values_h, wq_h, wk_h, wv_h, wg_h, wo_h, wu_h, wd_h,
    out,
    tok, lengths, head_gain, mixer_gain, final_gain, state, keys, values, factor, wp, wo, wu, wd, cosine, sine, offset,
    t_all, b1_out, b1_in0, b1_in1, b2_out, b2_in, retained, turned, heads, m_all, d_out, d_in,
    s_out, s_in, p_out, p_in, col_out, col_in, ends, lift, payload, hidden, h_all,
    g1_out, g1_inx, g1_iny, g2_out, g2_in, g_sum, act_all, e_out, e_in, j_out, j_in,
    local, send, r_w, r_a, r_b10, r_b11, r_b2, r_c, r_d, r_e, r_p, r_col, r_f,
    r_g1x, r_g1y, r_g2, r_h1, r_h2, r_i, r_j, r_x, r_v,
):
    y, x, z, c = [lax.axis_index(name) for name in AXES]
    kv = y * 4 + x
    sibling = (y, x, z, 1 - c)
    row_of = lax.rem(x, 2)
    owner = row_of == c
    pair = x // 2
    partner = (y, 2 * pair + 1 - row_of, z, c)
    pending = [None] * SENDS
    used = [0]

    def sent(slot):
        if pending[slot] is None:
            return
        when, copy = pending[slot]
        pending[slot] = None
        if when is None:
            copy.wait_send()
        else:

            @pl.when(when)
            def _():
                copy.wait_send()

    def put(src, dst, recv, device, when=None, slot=None):
        if slot is None:
            slot = used[0] % POOL
            used[0] += 1
        sent(slot)
        copy = copy_to(src, dst, send.at[slot], recv, device)
        if when is None:
            copy.start()
        else:

            @pl.when(when)
            def _():
                copy.start()

        pending[slot] = (when, copy)

    def settle():
        for slot in range(SENDS):
            sent(slot)

    def arrived(dst, sem, when=None):
        copy = copy_to(dst, dst, send.at[0], sem, sibling)
        if when is None:
            copy.wait_recv()
        else:

            @pl.when(when)
            def _():
                copy.wait_recv()

    barrier = pltpu.get_barrier_semaphore()
    greeted = 0
    for dy in range(4):
        for dx in range(4):
            for dc in range(2):
                if dy or dx or dc:
                    peer = (lax.rem(y + dy, 4), lax.rem(x + dx, 4), z, lax.rem(c + dc, 2))
                    pl.semaphore_signal(barrier, inc=1, device_id=peer, device_id_type=pl.DeviceIdType.MESH)
                    greeted += 1
    for dz in range(1, 8):
        peer = (y, x, lax.rem(z + dz, 8), c)
        pl.semaphore_signal(barrier, inc=1, device_id=peer, device_id_type=pl.DeviceIdType.MESH)
        greeted += 1
        peer = (y, 2 * pair + 1 - row_of, lax.rem(z + dz, 8), c)
        pl.semaphore_signal(barrier, inc=1, device_id=peer, device_id_type=pl.DeviceIdType.MESH)
        greeted += 1

    small = []
    for src, dst in (
        (lengths_h, lengths), (tok_h, tok), (head_gain_h, head_gain), (mixer_gain_h, mixer_gain),
        (final_gain_h, final_gain),
    ):
        small.append(pltpu.make_async_copy(src, dst, local.at[10 + len(small)]))
        small[-1].start()

    here = []

    def fetch(src, dst):
        here.append(pltpu.make_async_copy(src, dst, local.at[len(here)]))
        here[-1].start()

    quarter = [wp.at[c, :, pl.ds(128 * i, 128)] for i in range(4)]
    for src, dst in zip((wq_h, wk_h, wv_h, wg_h), quarter):
        fetch(src, dst)
    fetch(wo_h, wo.at[c])
    fetch(wu_h, wu.at[row_of, c])
    fetch(wd_h, wd.at[row_of, c])
    fetch(keys_h, keys)
    fetch(values_h, values)
    fetch(state_h, state)

    ones = jnp.full((8, 256), 1.0, B16)
    first = jnp.where(lax.broadcasted_iota(jnp.int32, (8, 256), 0) == 0, 1.0, 0.0).astype(B16)
    lane = lax.broadcasted_iota(jnp.int32, (64, 128), 1)
    low = lax.rem(lane, HDIM) < HDIM // 2
    lane_row = lax.broadcasted_iota(jnp.int32, (1, 128), 1)
    rate = jnp.where(lane_row < HDIM, rates[0], rates[1])

    def row_sums(u):
        total = None
        for _ in range(3):
            part = u.astype(B16)
            u = u - part.astype(F32)
            term = lax.dot_general(ones, part, (((1,), (1,)), ((), ())), preferred_element_type=F32)
            total = term if total is None else total + term
        return total

    def packed_sums(part_mean, part_centred):
        means = jnp.broadcast_to(part_mean * (1.0 / 256), (64, 256))
        return row_sums(jnp.concatenate([means, part_centred * part_centred], 0))

    def combined(own_sums, sums):
        total = jnp.sum(sums[...], axis=0)
        mean = total * (1.0 / 16)
        shift = jnp.where((lane_row < 64)[None], sums[...] - mean[None], 0.0)
        between = jnp.sum(shift * shift, axis=0)
        spread = (pltpu.roll(total, 64, 1) + 256.0 * between) * (1.0 / 4096)
        scale = jnp.where(lane_row < 64, lax.rsqrt(spread + EPS), 0.0)
        own_shift = jnp.broadcast_to(jnp.where(lane_row < 64, own_sums[...] - mean, 0.0), (8, 128))
        return shift, own_shift, jnp.broadcast_to(scale, (8, 128))

    def column(u):
        total = None
        for _ in range(3):
            part = u.astype(B16)
            u = u - part.astype(F32)
            term = lax.dot_general(part, first, (((0,), (0,)), ((), ())), preferred_element_type=F32)
            total = term if total is None else total + term
        return total

    small[0].wait()
    position = column(jnp.broadcast_to(lengths[...].astype(F32), (8, 64)))[:, :128]
    offset[...] = position - jnp.floor(position * (1.0 / BLK)) * BLK
    inverse = jnp.zeros((1, 128), F32)
    for i in range(HDIM // 2):
        inverse = jnp.where(lax.rem(lane_row, HDIM // 2) == i, 10000.0 ** (-i / (HDIM // 2)), inverse)
    angle = position * inverse
    cosine[...] = jnp.cos(angle)
    sines = jnp.sin(angle)
    sine[...] = jnp.where(low, -sines, sines)

    def decay(i, carry):
        rows = pl.ds(pl.multiple_of(i * 8, 8), 8)
        off = offset[rows, :][:, None, :]
        slot = lax.broadcasted_iota(jnp.int32, (8, BLK, 128), 1).astype(F32)
        lag = jnp.maximum(off - slot, 0.0)
        factor[rows] = jnp.where(slot < off, jnp.exp(-rate[None] * lag), 0.0)
        return carry

    lax.fori_loop(0, 8, decay, 0)
    for copy in small[1:]:
        copy.wait()
    t_all[z] = tok[...]
    pl.semaphore_wait(barrier, greeted)

    for d in (1, 7, 2, 6):
        put(tok, t_all.at[z], r_a.at[z], (y, x, lax.rem(z + d, 8), c))
    for i, (src, dst) in enumerate(
        [*zip((wq_h, wk_h, wv_h, wg_h), quarter), (wo_h, wo.at[c])]
    ):
        put(src, dst, r_w.at[max(i - 3, 0)], sibling)
    theirs = [wp.at[1 - c], wo.at[1 - c], wu.at[row_of, 1 - c], wd.at[row_of, 1 - c]]
    def chunk(k, side, core):
        if k < 2:
            return wu.at[side, core, pl.ds(128 * k, 128), :]
        return wd.at[side, core, pl.ds(512 * (k - 2), 512), :]

    def to_partner(k):
        put(chunk(k, row_of, c), chunk(k, row_of, c), r_x.at[k], partner, slot=POOL + k)

    def on_to_sibling(k):
        arrived(chunk(k, 1 - row_of, c), r_x.at[k])
        put(chunk(k, 1 - row_of, c), chunk(k, 1 - row_of, c), r_v.at[k], sibling)

    here[5].wait()
    to_partner(0)
    for i in range(4):
        here[i].wait()
    arrived(theirs[0], r_w.at[0])

    for d in NEAR:
        zp = lax.rem(z + 8 - d, 8)
        if d:
            arrived(t_all.at[zp], r_a.at[zp])
        for further in {2: (1, 2), 6: (7,)}.get(d, ()):
            put(t_all.at[zp], t_all.at[zp], r_a.at[zp], (y, x, lax.rem(z + further, 8), c))
        yd, side = zp // 2, lax.rem(zp, 2)
        xd = 2 * side + c
        rows = t_all[zp]
        for colour in range(2):
            part = dot(rows, wp[colour]).astype(B16)
            b1_out[zp, colour] = part
            if colour == 0:
                mine, dst, sem, to = xd == x, b1_in0.at[x, yd], r_b10.at[yd], (y, xd, z, c)
            else:
                mine, dst, sem, to = yd == y, b1_in1.at[y, side], r_b11.at[side], (yd, x, z, c)

            @pl.when(mine)
            def _():
                dst[...] = part

            put(b1_out.at[zp, colour], dst, sem, to, jnp.logical_not(mine))

    put(wu_h, wu.at[row_of, c], r_w.at[2], sibling)
    put(wd_h, wd.at[row_of, c], r_w.at[3], sibling)

    def first_stage_x(j):
        piece = lax.rem(z // 2 + j, 4)

        @pl.when(owner)
        def _():
            arrived(b1_in0.at[pl.ds(0, 3), piece], r_b10.at[piece])
            total = b1_in0[0, piece].astype(F32)
            for k in range(1, 4):
                total = total + b1_in0[k, piece].astype(F32)
            b2_out[j] = total.astype(B16)

        mine = jnp.logical_and(piece == y, c == 0)

        @pl.when(jnp.logical_and(owner, mine))
        def _():
            b2_in[y] = b2_out[j]

        put(
            b2_out.at[j], b2_in.at[y], r_b2.at[0], (piece, x, z, 0),
            jnp.logical_and(owner, jnp.logical_not(mine)),
        )

    def first_stage_y(j):
        side = lax.rem(z + j, 2)
        arrived(b1_in1.at[pl.ds(0, 3), side], r_b11.at[side])
        total = b1_in1[0, side].astype(F32)
        for k in range(1, 4):
            total = total + b1_in1[k, side].astype(F32)
        total = total.astype(B16)
        b2_out[4 + j] = total
        xd = 2 * side + c
        mine = jnp.logical_and(xd == x, c == 1)

        @pl.when(mine)
        def _():
            b2_in[x] = total

        put(b2_out.at[4 + j], b2_in.at[x], r_b2.at[0], (y, xd, z, 1), jnp.logical_not(mine))

    first_stage_x(0)
    first_stage_x(1)
    first_stage_y(0)
    first_stage_x(3)
    first_stage_y(1)
    first_stage_x(2)

    here[6].wait()
    to_partner(1)

    arrived(b2_in.at[pl.ds(0, 3)], r_b2.at[0], owner)
    arrived(b2_in, r_b2.at[0], jnp.logical_not(owner))
    qkvg = b2_in[0].astype(F32)
    for k in range(1, 4):
        qkvg = qkvg + b2_in[k].astype(F32)

    row_id = lax.broadcasted_iota(jnp.int32, (128, 128), 0)
    col_id = lax.broadcasted_iota(jnp.int32, (128, 128), 1)
    same_head = jnp.where(row_id // HDIM == col_id // HDIM, 1.0, 0.0).astype(B16)

    def rotated(u):
        partner = jnp.where(low, pltpu.roll(u, 96, 1), pltpu.roll(u, 32, 1))
        return u * cosine[...] + partner * sine[...]

    query, keyed, valued, gated = [
        qkvg[:, 128 * i : 128 * (i + 1)].astype(B16).astype(F32) for i in range(4)
    ]
    q_rot = rotated(query).astype(B16).astype(F32)
    k_rot = (rotated(keyed) * 0.125).astype(B16).astype(F32)
    own = split_dot(q_rot * k_rot, same_head, 2).astype(B16).astype(F32)
    turned[...] = q_rot
    retained[...] = own * valued
    for copy in here[7:]:
        copy.wait()
    pick_lane = lax.broadcasted_iota(jnp.int32, (HDIM, 128), 1)
    pick_row = lax.broadcasted_iota(jnp.int32, (HDIM, 128), 0)
    pick = jnp.where(lax.rem(pick_lane, HDIM) == pick_row, 1.0, 0.0)

    def attend(i, carry):
        rows = pl.ds(pl.multiple_of(i * 8, 8), 8)
        q = turned[rows, :]
        products = (keys[rows] * q.astype(B16)[:, None, :]).reshape(8 * BLK, 128)
        scores = dot(products, same_head).reshape(8, BLK, 128)
        weights = (scores * factor[rows]).astype(B16).astype(F32)
        inner = jnp.sum(weights * values[rows].astype(F32), axis=1)
        spread = (q[:, None, :] * pick[None]).reshape(8 * HDIM, 128).astype(B16)
        wide = dot(spread, same_head).reshape(8, HDIM, 128)
        cross = jnp.sum(wide * state[rows], axis=1)
        carried = jnp.exp(-rate * (offset[rows, :] + 1.0))
        retained[rows, :] += inner + cross * carried
        return carry

    lax.fori_loop(0, 8, attend, 0)
    kept = retained[...]
    centred = kept - split_dot(kept, same_head, 3) * (1.0 / HDIM)
    variance = split_dot(centred * centred, same_head, 3) * (1.0 / HDIM)
    normed = centred * lax.rsqrt(variance + EPS) * head_gain[...]
    mixed = (gated / (1.0 + jnp.exp(-gated)) * normed).astype(B16)
    heads[...] = mixed
    half = kv // 2

    for k in (10, 5, 7, 13, 15, 6, 14, 9, 11, 1, 4, 3, 12, 2, 8, 0):
        to = (lax.rem(y + k // 4, 4), lax.rem(x + k % 4, 4), z, row_of)
        put(heads, m_all.at[half, c], r_c.at[half], to, None if k else jnp.logical_not(owner))

    @pl.when(owner)
    def _():
        m_all[half, c] = mixed

    for k in range(2, 4):
        to_partner(k)
    on_to_sibling(0)

    here[4].wait()
    arrived(theirs[1], r_w.at[1])

    start = 2 * y + x // 2
    for j in (0, 1, 7, 2, 6, 3, 5, 4):
        i = lax.rem(start + j, 8)
        whole = 2 * i + c != kv
        arrived(m_all.at[i], r_c.at[i], whole)
        arrived(m_all.at[i, 0], r_c.at[i], jnp.logical_not(whole))
        part = (dot(m_all[i, 0], wo[0]) + dot(m_all[i, 1], wo[1])).astype(B16)
        mine = i == z

        @pl.when(mine)
        def _():
            d_in[i] = part

        d_out[i] = part
        put(d_out.at[i], d_in.at[z], r_d.at[0], (y, x, i, c), jnp.logical_not(mine))
    on_to_sibling(1)

    for i in (2, 3):
        arrived(theirs[i], r_w.at[i])
    gain_rows = jnp.broadcast_to(mixer_gain[...], (8, 256))
    for half in range(2):
        col_out[:, pl.ds(1024 * half, 1024)] = split_dot(gain_rows, wu[row_of, half], 3)[0:1]
    col_in[kv] = col_out[...]
    for k in (5, 7, 13, 15, 6, 14, 9, 11, 10, 1, 4, 3, 12, 2, 8):
        to = (lax.rem(y + k // 4, 4), lax.rem(x + k % 4, 4), z, c)
        put(col_out, col_in.at[kv], r_col.at[0], to)

    arrived(d_in.at[pl.ds(0, 7)], r_d.at[0])
    branch = d_in[z].astype(F32)
    for d in NEAR[1:]:
        i = lax.rem(z + 8 - d, 8)
        branch = branch + d_in[i].astype(F32)

    tall = ALPHA * tok[...].astype(F32) + branch
    part_mean = jnp.sum(tall, axis=1, keepdims=True) * (1.0 / 256)
    part_centred = tall - part_mean
    scaled = (part_centred * mixer_gain[...]).astype(B16)
    payload[...] = scaled
    turn = lax.rem(z, 2)
    stays = turn == row_of

    @pl.when(stays)
    def _():
        h_all[z // 2, row_of] = scaled

    for d in (4, 3, 5, 2, 6, 1, 7, 0):
        put(
            payload, h_all.at[z // 2, row_of], r_f.at[z // 2],
            (y, 2 * pair + turn, lax.rem(z + d, 8), c), None if d else jnp.logical_not(stays),
        )
    s_out[...] = packed_sums(part_mean, part_centred)[0:1]
    s_in[kv] = s_out[...]
    for k in (10, 5, 7, 13, 15, 6, 14, 9, 11, 1, 4, 3, 12, 2, 8):
        to = (lax.rem(y + k // 4, 4), lax.rem(x + k % 4, 4), z, c)
        put(s_out, s_in.at[kv], r_e.at[0], to)

    for k in range(2):
        arrived(chunk(k, 1 - row_of, 1 - c), r_v.at[k])

    along = (pair, y)
    size = (2, 4)

    def device_on(colour, stage, index):
        if (colour + stage) % 2 == 0:
            return (y, 2 * index + row_of, z, c)
        return (index, x, z, c)

    for d in range(4):
        t = lax.rem(z // 2 + (0, 1, 3, 2)[d], 4)
        whole = 2 * t + row_of != z
        arrived(h_all.at[t], r_f.at[t], whole)
        arrived(h_all.at[t, 0], r_f.at[t], jnp.logical_not(whole))
        for colour in range(2):
            part = (dot(h_all[t, 0], wu[0, colour]) + dot(h_all[t, 1], wu[1, colour])).astype(B16)
            for side in range(2):
                g1_out[colour, t, side] = part[32 * side : 32 * side + 32]
                spot = g1_out.at[colour, t, side]
                if colour == 0:
                    put(
                        spot, g1_inx.at[pair, t], r_g1x.at[t], device_on(0, 0, side),
                        pair != side,
                    )
                else:
                    put(spot, g1_iny.at[y, side], r_g1y.at[side], device_on(1, 0, t), y != t)

    arrived(s_in.at[pl.ds(0, 15)], r_e.at[0])
    shift, own_shift, scale = combined(s_out, s_in)
    eight = lax.broadcasted_iota(jnp.int32, (8, 128), 0)
    for group in range(2):
        stacked = jnp.zeros((8, 128), F32)
        for k in range(8):
            stacked = jnp.where(eight == k, shift[8 * group + k], stacked)
        p_out[group] = stacked
    p_out[2] = scale
    ends_at = 2 * y + row_of
    mine = ends_at == z

    @pl.when(mine)
    def _():
        p_in[...] = p_out[...]

    for d in range(1, 8):
        put(p_out, p_in, r_p.at[0], (y, x, lax.rem(z + d, 8), c), mine)
    wide_shift, wide_scale = column(own_shift)[:64], column(scale)[:64]
    hidden[...] = ((part_centred + wide_shift) * wide_scale * mixer_gain[...]).astype(B16)

    def first_sum(colour, j):
        me, other = along[colour], along[1 - colour]
        piece = lax.rem(other + j, size[1 - colour])
        total = (g1_out[0, piece, me] if colour == 0 else g1_out[1, me, piece]).astype(F32)
        if colour == 0:
            arrived(g1_inx.at[1 - pair, piece], r_g1x.at[piece])
            total = total + g1_inx[1 - pair, piece].astype(F32)
        else:
            arrived(g1_iny.at[pl.ds(0, 3), piece], r_g1y.at[piece])
            for d in (1, 3, 2):
                total = total + g1_iny[lax.rem(y + d, 4), piece].astype(F32)
        if j:
            g2_out[colour, piece] = total.astype(B16)
            put(
                g2_out.at[colour, piece], g2_in.at[colour, other], r_g2.at[colour],
                device_on(colour, 1, piece),
            )
        else:
            g_sum[colour] = total + lift[:, 1024 * colour : 1024 * colour + 1024]

    for colour, j in ((0, 2), (1, 1), (0, 1), (0, 3)):
        first_sum(colour, j)

    arrived(col_in.at[pl.ds(0, 15)], r_col.at[0])
    wide_eight = lax.broadcasted_iota(jnp.int32, (8, 2048), 0)
    arrived(p_in, r_p.at[0], jnp.logical_not(mine))
    lifted = jnp.zeros((128, 2048), F32)
    for group in range(2):
        stacked = jnp.zeros((8, 2048), F32)
        for k in range(8):
            stacked = jnp.where(wide_eight == k, col_in[8 * group + k], stacked)
        shift_high = p_in[group].astype(B16)
        shift_low = (p_in[group] - shift_high.astype(F32)).astype(B16)
        col_high = stacked.astype(B16)
        col_low = (stacked - col_high.astype(F32)).astype(B16)
        for a, b in ((shift_high, col_high), (shift_high, col_low), (shift_low, col_high)):
            lifted = lifted + lax.dot_general(a, b, (((0,), (0,)), ((), ())), preferred_element_type=F32)
    upper = pair == 1
    lift[...] = jnp.where(upper, lifted[32:64], lifted[:32])
    scales = column(p_in[2])
    ends[...] = jnp.where(upper, scales[32:64], scales[:32])

    for colour, j in ((0, 0), (1, 0)):
        first_sum(colour, j)
    for k in range(2, 4):
        on_to_sibling(k)

    def others(n):
        return (2, 1, 3) if n == 4 else (1,)

    for colour in range(2):
        me, other = along[colour], along[1 - colour]
        total = g_sum[colour]
        arrived(g2_in.at[colour, pl.ds(0, size[1 - colour] - 1)], r_g2.at[colour])
        for d in others(size[1 - colour]):
            source = lax.rem(other + d, size[1 - colour])
            total = total + g2_in[colour, source].astype(F32)
        times = jnp.concatenate([ends[...]] * 4, 1)
        active = jnp.square(jnp.maximum(total * times, 0.0)).astype(B16)
        spot = act_all.at[colour, y, pair]
        act_all[colour, y, pair] = active
        for stage in (1, 0):
            at = along[colour] if stage == 0 else along[1 - colour]
            n = size[(colour + stage) % 2]
            sem = r_h2.at[colour, y] if stage == 0 else r_h1.at[colour, other]
            for d in others(n):
                put(spot, spot, sem, device_on(colour, stage, lax.rem(at + d, n)))

    def forward(colour, j):
        me, other = along[colour], along[1 - colour]
        source = lax.rem(other + j, size[1 - colour])
        where = (source, pair) if colour == 0 else (y, source)
        spot = act_all.at[colour, where[0], where[1]]
        arrived(spot, r_h1.at[colour, source])
        for d in others(size[colour]):
            put(
                spot, spot, r_h2.at[colour, where[0]],
                device_on(colour, 0, lax.rem(me + d, size[colour])),
            )

    for colour, j in ((1, 1), (0, 1), (0, 3), (0, 2)):
        forward(colour, j)

    for k in range(2, 4):
        arrived(chunk(k, 1 - row_of, 1 - c), r_v.at[k])

    for j in range(4):
        t = y if j == 0 else j - 1 + (j - 1 >= y).astype(jnp.int32)
        arrived(act_all.at[0, t, 0], r_h2.at[0, t])
        if j:
            arrived(act_all.at[1, t], r_h2.at[1, t])
        upper_rows = act_all[0, t].reshape(64, 1024)
        lower_rows = act_all[1, t].reshape(64, 1024)
        for side in range(2):
            part = (dot(upper_rows, wd[side, 0]) + dot(lower_rows, wd[side, 1])).astype(B16)
            keep = jnp.logical_and(2 * t + row_of == z, row_of == side)
            e_out[t, side] = part

            @pl.when(keep)
            def _():
                e_in[z] = part

            put(
                e_out.at[t, side], e_in.at[z], r_i.at[0], (y, 2 * pair + side, 2 * t + row_of, c),
                jnp.logical_not(keep),
            )
    arrived(e_in.at[pl.ds(0, 7)], r_i.at[0], stays)
    arrived(e_in, r_i.at[0], jnp.logical_not(stays))
    downward = None
    for d in NEAR:
        i = lax.rem(z + 8 - d, 8)
        term = e_in[i].astype(F32)
        downward = term if downward is None else downward + term

    tall = ALPHA * hidden[...].astype(F32) + downward
    part_mean = jnp.sum(tall, axis=1, keepdims=True) * (1.0 / 256)
    part_centred = tall - part_mean
    j_out[...] = packed_sums(part_mean, part_centred)[0:1]
    j_in[kv] = j_out[...]
    for k in (10, 5, 7, 13, 15, 6, 14, 9, 11, 1, 4, 3, 12, 2, 8):
        to = (lax.rem(y + k // 4, 4), lax.rem(x + k % 4, 4), z, c)
        put(j_out, j_in.at[kv], r_j.at[0], to)
    arrived(j_in.at[pl.ds(0, 15)], r_j.at[0])
    shift, own_shift, scale = combined(j_out, j_in)
    wide_shift, wide_scale = column(own_shift)[:64], column(scale)[:64]
    out[...] = ((part_centred + wide_shift) * wide_scale * final_gain[...]).astype(B16)
    settle()


def per_device(
    tokens, lengths, state_block, cached_keys, cached_values, query_weight, key_weight,
    value_weight, gate_weight, decay_rate, head_gain, out_weight, mixer_gain, up_weight,
    down_weight, final_gain,
):
    vmem = pl.BlockSpec(memory_space=pltpu.VMEM)
    smem = pl.BlockSpec(memory_space=pltpu.SMEM)
    anywhere = pl.BlockSpec(memory_space=pl.ANY)
    dma = pltpu.SemaphoreType.DMA
    scratch = [
        pltpu.VMEM((64, 256), B16),
        pltpu.VMEM((1, 64), jnp.int32),
        pltpu.VMEM((1, 128), F32),
        pltpu.VMEM((1, 256), F32),
        pltpu.VMEM((1, 256), F32),
        pltpu.VMEM((64, 64, 128), F32),
        pltpu.VMEM((64, 128, 128), B16),
        pltpu.VMEM((64, 128, 128), B16),
        pltpu.VMEM((64, 128, 128), F32),
        pltpu.VMEM((2, 256, 512), B16),
        pltpu.VMEM((2, 128, 256), B16),
        pltpu.VMEM((2, 2, 256, 1024), B16),
        pltpu.VMEM((2, 2, 1024, 256), B16),
        pltpu.VMEM((64, 128), F32),
        pltpu.VMEM((64, 128), F32),
        pltpu.VMEM((64, 128), F32),
        pltpu.VMEM((8, 64, 256), B16),
        pltpu.VMEM((8, 2, 64, 512), B16),
        pltpu.VMEM((4, 4, 64, 512), B16),
        pltpu.VMEM((4, 2, 64, 512), B16),
        pltpu.VMEM((6, 64, 512), B16),
        pltpu.VMEM((4, 64, 512), B16),
        pltpu.VMEM((64, 128), F32),
        pltpu.VMEM((64, 128), F32),
        pltpu.VMEM((64, 128), B16),
        pltpu.VMEM((8, 2, 64, 128), B16),
        pltpu.VMEM((8, 64, 256), B16),
        pltpu.VMEM((8, 64, 256), B16),
        pltpu.VMEM((1, 128), F32),
        pltpu.VMEM((16, 1, 128), F32),
        pltpu.VMEM((3, 8, 128), F32),
        pltpu.VMEM((3, 8, 128), F32),
        pltpu.VMEM((1, 2048), F32),
        pltpu.VMEM((16, 1, 2048), F32),
        pltpu.VMEM((32, 256), F32),
        pltpu.VMEM((32, 2048), F32),
        pltpu.VMEM((64, 256), B16),
        pltpu.VMEM((64, 256), B16),
        pltpu.VMEM((4, 2, 64, 256), B16),
        pltpu.VMEM((2, 4, 2, 32, 1024), B16),
        pltpu.VMEM((2, 4, 32, 1024), B16),
        pltpu.VMEM((4, 2, 32, 1024), B16),
        pltpu.VMEM((2, 4, 32, 1024), B16),
        pltpu.VMEM((2, 4, 32, 1024), B16),
        pltpu.VMEM((2, 32, 1024), F32),
        pltpu.VMEM((2, 4, 2, 32, 1024), B16),
        pltpu.VMEM((4, 2, 64, 256), B16),
        pltpu.VMEM((8, 64, 256), B16),
        pltpu.VMEM((1, 128), F32),
        pltpu.VMEM((16, 1, 128), F32),
        dma((15,)),
        dma((SENDS,)),
        dma((4,)),
        dma((8,)),
        dma((4,)),
        dma((2,)),
        dma((1,)),
        dma((8,)),
        dma((1,)),
        dma((1,)),
        dma((1,)),
        dma((1,)),
        dma((4,)),
        dma((4,)),
        dma((2,)),
        dma((2,)),
        dma((2, 4)),
        dma((2, 4)),
        dma((1,)),
        dma((1,)),
        dma((4,)),
        dma((4,)),
    ]
    return pl.pallas_call(
        kernel,
        out_shape=jax.ShapeDtypeStruct((64, 256), B16),
        in_specs=[anywhere] * 5 + [smem] + [anywhere] * 10,
        out_specs=vmem,
        scratch_shapes=scratch,
        name="layer",
        compiler_params=pltpu.CompilerParams(
            collective_id=0, has_side_effects=True, vmem_limit_bytes=56 * 1024 * 1024
        ),
    )(
        tokens, lengths[None, :], head_gain[None, :], mixer_gain[None, :], final_gain[None, :], decay_rate,
        state_block, cached_keys, cached_values, query_weight, key_weight, value_weight, gate_weight,
        out_weight, up_weight, down_weight,
    )


def solution(mesh):
    finer = Mesh(mesh.devices.reshape(4, 4, 8, 2), AXES)
    kv, tp = ("y", "x"), ("z", "c")
    placed = (
        P(tp, kv), P(kv), P(kv, None, tp), P(kv, None, tp), P(kv, None, tp),
        P(kv, tp), P(kv, tp), P(kv, tp), P(kv, tp), P(tp), P(tp), P(tp, kv), P(kv),
        P(kv, tp), P(tp, kv), P(kv),
    )
    return jax.shard_map(per_device, mesh=finer, in_specs=placed, out_specs=P(tp, kv), check_vma=False)
```
